32 devices in a mesh: rep: 1, fs: 8 (over z, y), tp: 4 (over x, core).
Axes of the slice: x: 2, y: 2, z: 4, core: 2. Of those that a mesh axis runs over, the one named last changes fastest.
Arguments:
- tokens: bfloat16 [4096, 2048], P(('rep', 'fs')), may hold values from -6 to 6
- gate_outer: bfloat16 [2048, 1024], P('fs', 'tp'), may hold values from -0.125 to 0.125
- gate_inner: bfloat16 [2048, 1024], P('fs', 'tp'), may hold values from -0.125 to 0.125
- conv_input: bfloat16 [2048, 1024], P('fs', 'tp'), may hold values from -0.125 to 0.125
- mixer_output: bfloat16 [2048, 1024], P('fs', 'tp'), may hold values from -0.1875 to 0.1875
- conv_taps: float32 [3, 1024], P(None, 'tp'), may hold values from -3 to 3
- mixer_gain: float32 [2048], replicated, may hold values from 0.1 to 1.9
- mixer_shift: float32 [2048], replicated, may hold values from -3 to 3
- up_weight: bfloat16 [2048, 8192], P('fs', 'tp'), may hold values from -0.125 to 0.125
- down_weight: bfloat16 [2048, 8192], P('fs', 'tp'), may hold values from -0.0625 to 0.0625
- channel_gain: float32 [2048], replicated, may hold values from 0.1 to 1.9
- channel_shift: float32 [2048], replicated, may hold values from -3 to 3
Outputs:
- mixed: bfloat16 [4096, 2048], P(('rep', 'fs'))
The draws below stay inside these ranges and needn't reach their ends.
All inputs are finite; a program needn't handle non-finite values.
Results may differ from the reference program's by a relative error of at most 0.014.
Values may be sent and summed in bfloat16 or wider, within the bound.
A program may use at most 64 MiB of HBM per device.

```python
import jax
import jax.numpy as jnp
from jax import lax

D = 2048
C = 1024
FF = 8192
TAPS = 3
LEN = 512
SEQS = 8
TOKENS = 4096
N_TP = 4


def levels(rng, dims, shards, least, top_value):
    loudness = 1.0
    for axis_at, parts in shards:
        steps = jax.random.uniform(jax.random.fold_in(jax.random.fold_in(rng, 6), axis_at), (parts,), jnp.float32, least / len(shards), top_value / len(shards))
        loudness = loudness * jnp.repeat(jnp.exp(steps), dims[axis_at] // parts).reshape((-1,) + (1,) * (len(dims) - 1 - axis_at))
    return loudness


def bell_draw(own_key, dims, deviation, most, pieces=(), dtype=jnp.bfloat16):
    drawn = jax.random.normal(own_key, dims, jnp.float32) * deviation
    if len(pieces) > 0:
        drawn = levels(own_key, dims, pieces, -0.22, 0.18) * drawn
    return jnp.clip(drawn, min=-most, max=most).astype(dtype)


def setup_inputs(seed: int = 0) -> dict:
    arg_keys = jax.random.split(jax.random.key(seed), 13)
    return {
        "tokens": bell_draw(arg_keys[0], (TOKENS, D), 1.0, 6.0, ((0, 8),)),
        "gate_outer": bell_draw(arg_keys[1], (D, C), D ** -0.5, 0.125, ((0, 8), (1, 4))),
        "gate_inner": bell_draw(arg_keys[2], (D, C), D ** -0.5, 0.125, ((0, 8), (1, 4))),
        "conv_input": bell_draw(arg_keys[3], (D, C), D ** -0.5, 0.125, ((0, 8), (1, 4))),
        "mixer_output": bell_draw(arg_keys[4], (D, C), C ** -0.5, 0.1875, ((0, 8), (1, 4))),
        "conv_taps": bell_draw(arg_keys[5], (TAPS, C), 0.6, 3.0, ((1, 4),), jnp.float32),
        "mixer_gain": jnp.clip(1.0 + 0.18 * jax.random.normal(arg_keys[6], (D,), jnp.float32), 0.1, 1.9),
        "mixer_shift": bell_draw(arg_keys[7], (D,), 0.5, 3.0, (), jnp.float32),
        "up_weight": bell_draw(arg_keys[8], (D, FF), D ** -0.5, 0.125, ((0, 8), (1, 4))),
        "down_weight": bell_draw(arg_keys[9], (D, FF), FF ** -0.5, 0.0625, ((0, 8), (1, 4))),
        "channel_gain": jnp.clip(1.0 + 0.18 * jax.random.normal(arg_keys[10], (D,), jnp.float32), 0.1, 1.9),
        "channel_shift": bell_draw(arg_keys[11], (D,), 0.5, 3.0, (), jnp.float32),
    }


residual_scale = 8.0 ** 0.25
norm_epsilon = 1e-05

def layer_norm(values, gain, shift):
    row_mean = lax.optimization_barrier(jnp.mean(values, -1, keepdims=True))
    centered = values - row_mean
    variance = lax.optimization_barrier(jnp.mean(centered * centered, -1, keepdims=True))
    return centered * lax.rsqrt(variance + norm_epsilon) * gain + shift

def blockwise_sum(left, right_t):
    block_width = left.shape[1] // N_TP
    totals = jnp.zeros((left.shape[0], right_t.shape[0]), jnp.float32)
    for block_index in range(N_TP):
        lower = block_index * block_width
        product = lax.dot_general(left[:, lower:lower + block_width], right_t[:, lower:lower + block_width], (((1,), (1,)), ((), ())), preferred_element_type=jnp.float32)
        totals = totals + lax.optimization_barrier(product.astype(jnp.bfloat16)).astype(jnp.float32)
    return totals

def reference(tokens, gate_outer, gate_inner, conv_input, mixer_output, conv_taps, mixer_gain, mixer_shift, up_weight, down_weight, channel_gain, channel_shift):

    def one_sequence(seq_rows):
        outer_gate = jnp.dot(seq_rows, gate_outer, preferred_element_type=jnp.float32)
        inner_gate = jnp.dot(seq_rows, gate_inner, preferred_element_type=jnp.float32)
        conv_values = jnp.dot(seq_rows, conv_input, preferred_element_type=jnp.float32)
        product = inner_gate * conv_values
        padded = jnp.pad(product, ((TAPS - 1, 0), (0, 0)))
        result = jnp.zeros_like(product)
        for tap_index in range(TAPS):
            result = result + conv_taps[tap_index] * padded[tap_index:tap_index + LEN]
        conv_out = (outer_gate * result).astype(jnp.bfloat16)
        mixer_sum = blockwise_sum(conv_out, mixer_output)
        first = layer_norm(residual_scale * seq_rows.astype(jnp.float32) + mixer_sum, mixer_gain, mixer_shift).astype(jnp.bfloat16)
        up_product = jnp.dot(first, up_weight, preferred_element_type=jnp.float32)
        hidden = jnp.square(jax.nn.relu(up_product)).astype(jnp.bfloat16)
        channel_sum = blockwise_sum(hidden, down_weight)
        return layer_norm(residual_scale * first.astype(jnp.float32) + channel_sum, channel_gain, channel_shift).astype(jnp.bfloat16)
    sequences = tokens.reshape(SEQS, LEN, D)
    outputs = lax.map(one_sequence, sequences)
    return outputs.reshape(TOKENS, D)
```

```python
import functools

import jax
import jax.numpy as jnp
from jax import lax
from jax.experimental import pallas as pl
from jax.experimental.pallas import tpu as pltpu
from jax.sharding import PartitionSpec as P

residual_scale = 8.0**0.25
norm_epsilon = 1e-05
MESH = pl.DeviceIdType.MESH
f32 = jnp.float32
bf16 = jnp.bfloat16
NT = (((1,), (1,)), ((), ()))


def layer_norm(values, gain, shift):
    row_mean = jnp.mean(values, -1, keepdims=True)
    centered = values - row_mean
    variance = jnp.mean(centered * centered, -1, keepdims=True)
    return centered * lax.rsqrt(variance + norm_epsilon) * gain + shift


def xor(value, mask):
    bit = 1
    while bit <= mask:
        if mask & bit:
            value = value + bit - 2 * bit * ((value // bit) % 2)
        bit *= 2
    return value


def kernel(
    n_fs,
    n_tp,
    via,
    sub,
    tokens,
    w_go,
    w_gi,
    w_ci,
    w_mo,
    taps,
    m_gain,
    m_shift,
    w_up,
    w_dn,
    c_gain,
    c_shift,
    out,
    mix_g,
    up_g,
    dn_g,
    outer,
    zpad,
    conv,
    part,
    recv,
    first,
    hidden,
    part2,
    r_core,
    r_mate,
    r_x,
    result,
    local_sem,
    out_sem,
    gs_send,
    gs_recv,
    z_sends,
    y_sends,
    f_recv,
    t_send,
    t_recv,
    s1_send,
    s1_recv,
    s2_send,
    s2_recv,
    s3_send,
    s3_recv,
    o_send,
    o_recv,
):
    seq, width = tokens.shape
    rows = w_up.shape[0]
    units = w_up.shape[1]
    half = units // 2
    bits = n_tp.bit_length() - 1
    nk = n_fs // 2
    f = lax.axis_index("fs")
    t = lax.axis_index("tp")
    k = f // 2
    p = f % 2
    partner = f + 1 - 2 * p
    e = k % 2
    mate_k = k + 1 - 2 * e
    mate = 2 * mate_k + p
    core = t % 2
    hs = seq // 2
    has_right = k < nk - 1
    has_left = k > 0

    def flip(bit):
        return t + bit - 2 * bit * ((t // bit) % 2)

    def block(s):
        return pl.ds(pl.multiple_of(s * rows, rows), rows)

    own = block(f)
    copies = []
    for j, ref in enumerate((w_go, w_gi, w_ci, w_mo)):
        copies.append(pltpu.make_async_copy(ref, mix_g.at[j, own], local_sem.at[j]))
    keep_cols = pl.ds(pl.multiple_of(e * half, half), half)
    for j, (w, g) in enumerate(((w_up, up_g), (w_dn, dn_g))):
        copies.append(pltpu.make_async_copy(w.at[:, keep_cols], g.at[own], local_sem.at[4 + j]))
    for c in copies:
        c.start()

    barrier = pltpu.get_barrier_semaphore()
    pl.semaphore_signal(barrier, inc=1, device_id={"fs": partner}, device_id_type=MESH)
    for i in range(1, nk):
        pl.semaphore_signal(
            barrier, inc=1, device_id={"fs": 2 * xor(k, i) + p}, device_id_type=MESH
        )
    for b in range(bits):
        pl.semaphore_signal(barrier, inc=1, device_id={"tp": flip(1 << b)}, device_id_type=MESH)
    pl.semaphore_wait(barrier, nk + bits)

    for c in copies:
        c.wait()

    spans = ((0, rows - via), (rows - via, via))

    def piece(s, q):
        lo, n = spans[q]
        return mix_g.at[:, pl.ds(pl.multiple_of(s * rows + lo, 16), n)]

    def copy(s, q, way):
        ref = piece(s, q)
        return pltpu.make_async_remote_copy(
            src_ref=ref,
            dst_ref=ref,
            send_sem=gs_send.at[s, q, way],
            recv_sem=gs_recv.at[s, q],
            device_id={"fs": (partner, f + 2, f - 2)[way]},
            device_id_type=MESH,
        )

    def send(s, q, way):
        if way == 0:
            copy(s, q, 0).start()
        else:

            @pl.when(has_right if way == 1 else has_left)
            def _():
                copy(s, q, way).start()

    def arrive(s, q):
        copy(s, q, 0).wait_recv()

    def sides(d):
        return ((1, f - 2 * d, k - d >= 0), (2, f + 2 * d, k + d < nk))

    def begin():
        for q in (0, 1):
            for way in (0, 1, 2):
                send(f, q, way)

    def after_pair():
        arrive(partner, 0)
        send(partner, 0, 1)
        send(partner, 0, 2)

    def step(d):
        for way, s, ok in sides(d):

            @pl.when(ok)
            def _(way=way, s=s):
                other = s + 1 - 2 * p
                for q in (1, 0):
                    arrive(s, q)
                    if q == 1:
                        send(s, q, 0)
                    send(s, q, way)
                arrive(other, 0)
                send(other, 0, way)

    def finish():
        arrive(partner, 1)
        for d in range(1, nk):
            for way, s, ok in sides(d):

                @pl.when(ok)
                def _(s=s):
                    arrive(s + 1 - 2 * p, 1)

    def drain():
        for q in (0, 1):
            copy(f, q, 0).wait_send()
            for way, has in ((1, has_right), (2, has_left)):

                @pl.when(has)
                def _(q=q, way=way):
                    copy(f, q, way).wait_send()
                    if q == 0:
                        copy(partner, q, way).wait_send()

        for d in range(1, nk):
            for way, s, ok in sides(d):

                @pl.when(ok)
                def _(way=way, s=s):
                    copy(s, 1, 0).wait_send()

                    @pl.when(has_right if way == 1 else has_left)
                    def _():
                        copy(s, 0, way).wait_send()
                        copy(s, 1, way).wait_send()
                        copy(s + 1 - 2 * p, 0, way).wait_send()

    pairs = ((w_up, up_g), (w_dn, dn_g))

    def z_copy(a, to_k):
        w, g = pairs[a]
        cols = pl.ds(pl.multiple_of((to_k % 2) * half, half), half)
        return pltpu.make_async_remote_copy(
            src_ref=w.at[:, cols],
            dst_ref=g.at[own],
            send_sem=z_sends.at[a, to_k],
            recv_sem=f_recv.at[a, f],
            device_id={"fs": 2 * to_k + p},
            device_id_type=MESH,
        )

    def y_copy(a, of_k):
        ref = pairs[a][1].at[block(2 * of_k + p)]
        return pltpu.make_async_remote_copy(
            src_ref=ref,
            dst_ref=ref,
            send_sem=y_sends.at[a, of_k],
            recv_sem=f_recv.at[a, 2 * of_k + p],
            device_id={"fs": partner},
            device_id_type=MESH,
        )

    def f_wait(a, s):
        ref = pairs[a][1].at[block(s)]
        pltpu.make_async_remote_copy(
            src_ref=ref,
            dst_ref=ref,
            send_sem=y_sends.at[a, 0],
            recv_sem=f_recv.at[a, s],
            device_id={"fs": partner},
            device_id_type=MESH,
        ).wait_recv()

    def z_right(a, d):
        @pl.when(k == d)
        def _():
            for kk in range(d + 1, nk):
                z_copy(a, kk).start()

    def z_left(a, d):
        @pl.when(k == d)
        def _():
            for kk in range(d - 1, -1, -1):
                z_copy(a, kk).start()

    def z_all(a):
        for d in range(nk):
            z_right(a, d)
            z_left(a, d)

    def relay(a, of_k):
        f_wait(a, 2 * of_k + p)
        y_copy(a, of_k).start()

    def f_drain(a):
        for kk in range(nk):
            y_copy(a, kk).wait_send()

            @pl.when(k != kk)
            def _(kk=kk):
                z_copy(a, kk).wait_send()

    group = k // 2
    order = [2 * group, 2 * group + 1]
    for m in range(1, nk // 2):
        low = (group // (1 << (m.bit_length() - 1))) % 2
        for j in (0, 1):
            order.append(2 * xor(group, m) + low * (1 - j) + (1 - low) * j)
    relays = [mate_k] + order[2:]

    starts = [0]
    for b in range(bits):
        starts.append(starts[-1] + ((t // (1 << b)) % 2) * (seq >> (b + 1)))

    def aways(b):
        return starts[b] + (1 - (t // (1 << b)) % 2) * (seq >> (b + 1))

    def span(start, n):
        return pl.ds(pl.multiple_of(start, n), n)

    def t_copy(i, src, dst, device):
        return pltpu.make_async_remote_copy(
            src_ref=src,
            dst_ref=dst,
            send_sem=t_send.at[i],
            recv_sem=t_recv.at[i],
            device_id=device,
            device_id_type=MESH,
        )

    def landing(b):
        return seq - (seq >> b)

    def reduce_copy(b):
        n = seq >> (b + 1)
        return t_copy(
            b, part.at[span(aways(b), n)], recv.at[pl.ds(landing(b), n)], {"tp": flip(1 << b)}
        )

    def add_recv(b, start, n):
        base = landing(b) - starts[b + 1]
        tile = min(n, 16)

        @pl.loop(0, n // tile)
        def _(i):
            mine = pl.ds(pl.multiple_of(start + i * tile, tile), tile)
            theirs = pl.ds(pl.multiple_of(base + start + i * tile, tile), tile)
            part[mine] = (part[mine].astype(f32) + recv[theirs].astype(f32)).astype(bf16)

    def gather_copy(i, q, b):
        ref = first.at[q, span(starts[b + 1], seq >> (b + 1))]
        return t_copy(i + b, ref, ref, {"tp": flip(1 << b)})

    begin()
    after_pair()
    z_right(0, 0)
    z_left(0, nk - 1)
    for d in range(1, nk):
        step(d)
        z_right(0, d)
        z_left(0, nk - 1 - d)
    y_copy(0, k).start()
    finish()

    pad = zpad.shape[0] - seq
    zpad[0:pad] = jnp.zeros((pad, zpad.shape[1]), f32)
    tile = seq // 2

    @pl.loop(0, 2)
    def _(i):
        at = pl.ds(pl.multiple_of(i * tile, tile), tile)
        x = tokens[at]
        outer[at] = jnp.dot(x, mix_g[0], preferred_element_type=f32)
        inner = jnp.dot(x, mix_g[1], preferred_element_type=f32)
        values = jnp.dot(x, mix_g[2], preferred_element_type=f32)
        zpad[pl.ds(pl.multiple_of(i * tile + pad, 8), tile)] = inner * values

    n_taps = taps.shape[0]
    acc = jnp.zeros((seq, zpad.shape[1]), f32)
    for j in range(n_taps):
        lo = pad - (n_taps - 1) + j
        acc = acc + taps[j : j + 1] * zpad[lo : lo + seq]
    conv[...] = (outer[...] * acc).astype(bf16)
    wide = min(256, width)

    def mix_out(start):
        at_rows = span(start, hs)
        lhs = conv[at_rows]

        @pl.loop(0, width // wide)
        def _(i):
            at = pl.ds(pl.multiple_of(i * wide, wide), wide)
            part[at_rows, at] = lax.dot_general(
                lhs, mix_g[3, at], NT, preferred_element_type=f32
            ).astype(bf16)

    mix_out(aways(0))
    reduces = [reduce_copy(b) for b in range(bits)]
    reduces[0].start()
    mix_out(starts[1])
    relay(0, relays[0])
    for b in range(1, bits):
        n = seq >> (b + 1)
        reduces[b - 1].wait_recv()
        add_recv(b - 1, aways(b), n)
        reduces[b].start()
        add_recv(b - 1, starts[b + 1], n)
    if nk > 2:
        relay(0, relays[1])
    last = bits - 1
    reduces[last].wait_recv()
    n_own = seq >> bits
    tile_n = min(n_own, 16)

    @pl.loop(0, n_own // tile_n)
    def _(i):
        at = pl.ds(pl.multiple_of(starts[bits] + i * tile_n, tile_n), tile_n)
        theirs = pl.ds(pl.multiple_of(landing(last) + i * tile_n, tile_n), tile_n)
        total = part[at].astype(f32) + recv[theirs].astype(f32)
        first[e, at] = layer_norm(
            residual_scale * tokens[at].astype(f32) + total, m_gain[...], m_shift[...]
        ).astype(bf16)

    mine_n = first.at[e, span(starts[bits], n_own)]
    to_mate = t_copy(bits, mine_n, mine_n, {"fs": mate})
    own_g = [gather_copy(bits + 1, e, b) for b in range(bits)]
    mate_g = [gather_copy(2 * bits + 1, 1 - e, b) for b in range(bits)]
    to_mate.start()
    own_g[last].start()
    z_all(1)
    for m in relays[2:-1]:
        relay(0, m)
    for b in range(last, 0, -1):
        own_g[b].wait_recv()
        own_g[b - 1].start()
    to_mate.wait_recv()
    mate_g[last].start()
    if nk > 2:
        relay(0, relays[-1])
    y_copy(1, k).start()
    own_g[0].wait_recv()
    f_wait(0, partner)
    for m in relays:
        f_wait(0, 2 * m + 1 - p)

    wide_u = min(256, half)

    def up(q):
        @pl.loop(0, half // wide_u)
        def _(i):
            at = pl.ds(pl.multiple_of(i * wide_u, wide_u), wide_u)
            u = jnp.maximum(jnp.dot(first[q], up_g[:, at], preferred_element_type=f32), 0.0)
            hidden[q, :, at] = (u * u).astype(bf16)

    up(e)
    for b in range(last, 0, -1):
        mate_g[b].wait_recv()
        mate_g[b - 1].start()
    relay(1, relays[0])
    mate_g[0].wait_recv()
    up(1 - e)

    cw = 2 * rows // sub
    mine_h = pl.ds(pl.multiple_of(core * hs, hs), hs)
    away_h = pl.ds(pl.multiple_of((1 - core) * hs, hs), hs)
    chunks = []
    for m in order:
        if sub == 2:
            chunks.append((m, (2 * m + p) * rows))
            chunks.append((m, (2 * m + 1 - p) * rows))
        else:
            chunks.append((m, 2 * m * rows))

    def cols_of(j):
        return pl.ds(pl.multiple_of(chunks[j][1], cw), cw)

    def remote(src, dst, ssem, rsem, device):
        return pltpu.make_async_remote_copy(
            src_ref=src,
            dst_ref=dst,
            send_sem=ssem,
            recv_sem=rsem,
            device_id=device,
            device_id_type=MESH,
        )

    def s1(j):
        c = cols_of(j)
        return remote(
            part2.at[:, away_h, c],
            r_core.at[:, :, c],
            s1_send.at[j],
            s1_recv.at[j],
            {"tp": flip(1)},
        )

    def s2(j):
        c = cols_of(j)
        return remote(
            part2.at[1 - e, mine_h, c],
            r_mate.at[:, c],
            s2_send.at[j],
            s2_recv.at[j],
            {"fs": mate},
        )

    def s3(j, b):
        c = cols_of(j)
        return remote(
            part2.at[e, mine_h, c],
            r_x.at[b - 1, :, c],
            s3_send.at[b - 1, j],
            s3_recv.at[b - 1, j],
            {"tp": flip(1 << b)},
        )

    def product(j):
        c = cols_of(j)
        w = dn_g[c]

        @pl.loop(0, 2)
        def _(q):
            part2[q, :, c] = lax.dot_general(
                hidden[q], w, NT, preferred_element_type=f32
            ).astype(bf16)

        s1(j).start()

    def core_sum(j):
        c = cols_of(j)
        s1(j).wait_recv()
        part2[1 - e, mine_h, c] = (
            part2[1 - e, mine_h, c].astype(f32) + r_core[1 - e, :, c].astype(f32)
        ).astype(bf16)
        s2(j).start()

    def mate_sum(j):
        c = cols_of(j)
        s2(j).wait_recv()
        part2[e, mine_h, c] = (
            part2[e, mine_h, c].astype(f32)
            + r_core[e, :, c].astype(f32)
            + r_mate[:, c].astype(f32)
        ).astype(bf16)
        s3(j, 1).start()

    def x_sum(j, b):
        c = cols_of(j)
        s3(j, b - 1).wait()
        part2[e, mine_h, c] = (
            part2[e, mine_h, c].astype(f32) + r_x[b - 2, :, c].astype(f32)
        ).astype(bf16)
        s3(j, b).start()

    stages = [core_sum, mate_sum]
    for b in range(2, bits):
        stages.append(functools.partial(x_sum, b=b))
    n_ch = len(chunks)

    def advance(j):
        for i, stage in enumerate(stages):
            if 0 <= j - 1 - i < n_ch:
                stage(j - 1 - i)

    def arrived(j):
        m = chunks[j][0]
        if sub == 1:
            f_wait_other(m, 0)
            f_wait_other(m, 1)
        else:
            f_wait_other(m, j % 2)

    def f_wait_other(m, other):
        if other:
            f_wait(1, 2 * m + 1 - p)

    for j in range(n_ch):
        n = j // sub
        if n >= 1 and j % sub == sub - 1 and n + 1 < nk:
            relay(1, order[n + 1])
        if sub == 1 and n == 1 and nk > 2:
            pass
        arrived(j)
        product(j)
        advance(j)
    for j in range(n_ch, n_ch + len(stages)):
        advance(j)

    n_out = o_send.shape[0]
    piece_rows = hs // n_out
    tile_o = min(piece_rows, 16)

    def out_rows(i):
        return pl.ds(pl.multiple_of(core * hs + i * piece_rows, piece_rows), piece_rows)

    def out_local(i):
        return pltpu.make_async_copy(
            result.at[pl.ds(i * piece_rows, piece_rows)], out.at[out_rows(i)], out_sem.at[i]
        )

    def out_remote(i):
        return remote(
            result.at[pl.ds(i * piece_rows, piece_rows)],
            out.at[out_rows(i)],
            o_send.at[i],
            o_recv.at[i],
            {"tp": flip(1)},
        )

    for j in range(n_ch):
        s3(j, last).wait_recv()
    for i in range(n_out):

        @pl.loop(0, piece_rows // tile_o)
        def _(ii):
            lo = i * piece_rows + ii * tile_o
            here = pl.ds(pl.multiple_of(lo, tile_o), tile_o)
            at = pl.ds(pl.multiple_of(core * hs + lo, tile_o), tile_o)
            total = part2[e, at].astype(f32) + r_x[last - 1, here].astype(f32)
            result[here] = layer_norm(
                residual_scale * first[e, at].astype(f32) + total, c_gain[...], c_shift[...]
            ).astype(bf16)

        out_local(i).start()
        out_remote(i).start()

    drain()
    f_drain(0)
    f_drain(1)
    for c in reduces + [to_mate] + own_g + mate_g:
        c.wait_send()
    for j in range(n_ch):
        s1(j).wait_send()
        s2(j).wait_send()
        s3(j, last).wait_send()
    for i in range(n_out):
        out_local(i).wait()
        out_remote(i).wait()


def local(
    tokens,
    gate_outer,
    gate_inner,
    conv_input,
    mixer_output,
    conv_taps,
    mixer_gain,
    mixer_shift,
    up_weight,
    down_weight,
    channel_gain,
    channel_shift,
):
    seq, width = tokens.shape
    rows, units = up_weight.shape
    chans = gate_outer.shape[1]
    half = units // 2
    n_fs = lax.axis_size("fs")
    n_tp = lax.axis_size("tp")
    bits = n_tp.bit_length() - 1
    nk = n_fs // 2
    via = max(16, rows * 13 // 16 // 16 * 16)
    sub = 2 if rows % 128 == 0 else 1
    n_ch = nk * sub
    hs = seq // 2
    n_out = 4
    n_t = 3 * bits + 1
    vmem = pl.BlockSpec(memory_space=pltpu.VMEM)
    dma = pltpu.SemaphoreType.DMA
    return pl.pallas_call(
        functools.partial(kernel, n_fs, n_tp, via, sub),
        out_shape=jax.ShapeDtypeStruct((seq, width), bf16),
        in_specs=[vmem] * 12,
        out_specs=pl.BlockSpec(memory_space=pl.ANY),
        scratch_shapes=[
            pltpu.VMEM((4, width, chans), bf16),
            pltpu.VMEM((width, half), bf16),
            pltpu.VMEM((width, half), bf16),
            pltpu.VMEM((seq, chans), f32),
            pltpu.VMEM((seq + 8, chans), f32),
            pltpu.VMEM((seq, chans), bf16),
            pltpu.VMEM((seq, width), bf16),
            pltpu.VMEM((seq, width), bf16),
            pltpu.VMEM((2, seq, width), bf16),
            pltpu.VMEM((2, seq, half), bf16),
            pltpu.VMEM((2, seq, width), bf16),
            pltpu.VMEM((2, hs, width), bf16),
            pltpu.VMEM((hs, width), bf16),
            pltpu.VMEM((bits - 1, hs, width), bf16),
            pltpu.VMEM((hs, width), bf16),
            dma((6,)),
            dma((n_out,)),
            dma((n_fs, 2, 3)),
            dma((n_fs, 2)),
            dma((2, nk)),
            dma((2, nk)),
            dma((2, n_fs)),
            dma((n_t,)),
            dma((n_t,)),
            dma((n_ch,)),
            dma((n_ch,)),
            dma((n_ch,)),
            dma((n_ch,)),
            dma((bits - 1, n_ch)),
            dma((bits - 1, n_ch)),
            dma((n_out,)),
            dma((n_out,)),
        ],
        compiler_params=pltpu.CompilerParams(
            collective_id=0, has_side_effects=True, vmem_limit_bytes=62 * 1024 * 1024
        ),
    )(
        tokens,
        gate_outer,
        gate_inner,
        conv_input,
        mixer_output,
        conv_taps,
        mixer_gain.reshape(1, width),
        mixer_shift.reshape(1, width),
        up_weight,
        down_weight,
        channel_gain.reshape(1, width),
        channel_shift.reshape(1, width),
    )


def solution(mesh):
    in_specs = (
        P(("rep", "fs"), None),
        P("fs", "tp"),
        P("fs", "tp"),
        P("fs", "tp"),
        P("fs", "tp"),
        P(None, "tp"),
        P(),
        P(),
        P("fs", "tp"),
        P("fs", "tp"),
        P(),
        P(),
    )
    out_specs = P(("rep", "fs"), None)
    return jax.shard_map(local, mesh=mesh, in_specs=in_specs, out_specs=out_specs, check_vma=False)
```

```python
import functools

import jax
import jax.numpy as jnp
from jax import lax
from jax.experimental import pallas as pl
from jax.experimental.pallas import tpu as pltpu
from jax.sharding import PartitionSpec as P

residual_scale = 8.0**0.25
norm_epsilon = 1e-05
MESH = pl.DeviceIdType.MESH
f32 = jnp.float32
bf16 = jnp.bfloat16
NT = (((1,), (1,)), ((), ()))


def layer_norm(values, gain, shift):
    row_mean = jnp.mean(values, -1, keepdims=True)
    centered = values - row_mean
    variance = jnp.mean(centered * centered, -1, keepdims=True)
    return centered * lax.rsqrt(variance + norm_epsilon) * gain + shift


def xor(value, mask):
    bit = 1
    while bit <= mask:
        if mask & bit:
            value = value + bit - 2 * bit * ((value // bit) % 2)
        bit *= 2
    return value


def kernel(
    n_fs,
    n_tp,
    sub,
    n_pc,
    hops,
    tokens,
    w_go,
    w_gi,
    w_ci,
    w_mo,
    taps,
    m_gain,
    m_shift,
    w_up,
    w_dn,
    c_gain,
    c_shift,
    out,
    mix_g,
    up_g,
    dn_g,
    tok_m,
    outer,
    zpad,
    conv,
    part,
    recv,
    r_sum,
    first,
    hidden,
    part2,
    r_core,
    r_mate,
    r_x,
    result,
    local_sem,
    out_sem,
    z_sends,
    y_sends,
    f_recv,
    t_send,
    t_recv,
    s1_send,
    s1_recv,
    s2_send,
    s2_recv,
    s3_send,
    s3_recv,
    o_send,
    o_recv,
):
    seq, width = tokens.shape
    rows = w_up.shape[0]
    half = w_up.shape[1] // 2
    hc = mix_g.shape[2]
    bits = n_tp.bit_length() - 1
    nk = n_fs // 2
    f = lax.axis_index("fs")
    t = lax.axis_index("tp")
    k = f // 2
    p = f % 2
    partner = f + 1 - 2 * p
    e = k % 2
    mate_k = k + 1 - 2 * e
    mate = 2 * mate_k + p
    core = t % 2
    hs = seq // 2
    inner = jnp.logical_and(k > 0, k < nk - 1)

    def flip(bit):
        return t + bit - 2 * bit * ((t // bit) % 2)

    def span(start, n):
        return pl.ds(pl.multiple_of(start, n), n)

    def remote(src, dst, ssem, rsem, device):
        return pltpu.make_async_remote_copy(
            src_ref=src,
            dst_ref=dst,
            send_sem=ssem,
            recv_sem=rsem,
            device_id=device,
            device_id_type=MESH,
        )

    sources = (w_go, w_gi, w_ci, w_mo, w_up, w_dn)
    UP, DN = 4, 5

    def pieces(a):
        return n_pc if a >= UP else 1

    def source(a, parity, q):
        w = sources[a]
        pn = rows // pieces(a)
        at = pl.ds(q * pn, pn)
        if len(w.shape) == 3:
            return w.at[parity, at]
        n = half if a >= UP else hc
        return w.at[at, span(parity * n, n)]

    def held(a, s, q):
        pn = rows // pieces(a)
        at = span(s * rows + q * pn, pn)
        if a < UP:
            return mix_g.at[a, at]
        return (up_g if a == UP else dn_g).at[at]

    copies = []
    for a in range(6):
        for q in range(pieces(a)):
            copies.append(
                pltpu.make_async_copy(source(a, e, q), held(a, f, q), local_sem.at[a, q])
            )
    for c in copies:
        c.start()

    barrier = pltpu.get_barrier_semaphore()
    pl.semaphore_signal(barrier, inc=1, device_id={"fs": partner}, device_id_type=MESH)
    for i in range(1, nk):
        pl.semaphore_signal(
            barrier, inc=1, device_id={"fs": 2 * xor(k, i) + p}, device_id_type=MESH
        )
    for b in range(bits):
        pl.semaphore_signal(barrier, inc=1, device_id={"tp": flip(1 << b)}, device_id_type=MESH)
    pl.semaphore_wait(barrier, nk + bits)

    def z_copy(a, to_k, q):
        return remote(
            source(a, to_k % 2, q),
            held(a, f, q),
            z_sends.at[a, to_k, q],
            f_recv.at[a, f, q],
            {"fs": 2 * to_k + p},
        )

    def y_copy(a, of_k, q):
        ref = held(a, 2 * of_k + p, q)
        return remote(
            ref, ref, y_sends.at[a, of_k, q], f_recv.at[a, 2 * of_k + p, q], {"fs": partner}
        )

    def f_wait(a, s, q):
        ref = held(a, s, q)
        remote(ref, ref, y_sends.at[a, 0, q], f_recv.at[a, s, q], {"fs": partner}).wait_recv()

    def z_send(a, kk):
        for q in range(pieces(a)):
            z_copy(a, kk, q).start()

    def z_right(arrays, d, lo=1, hi=None):
        @pl.when(k == d)
        def _():
            for kk in range(d + lo, nk if hi is None else min(d + hi, nk)):
                for a in arrays:
                    z_send(a, kk)

    def z_left(arrays, d, lo=1, hi=None):
        @pl.when(k == d)
        def _():
            for kk in range(d - lo, -1 if hi is None else max(d - hi, -1), -1):
                for a in arrays:
                    z_send(a, kk)

    def z_all(arrays):
        for d in range(nk):
            z_right(arrays, d)
            z_left(arrays, d)

    def z_ends(arrays, lo, hi=None):
        z_right(arrays, 0, lo, hi)
        z_left(arrays, nk - 1, lo, hi)

    def z_mid(arrays, lo=1, hi=None):
        for d in range(1, nk - 1):
            if d < nk - 2:
                z_right(arrays, d, lo, hi)
            if d > 1:
                z_left(arrays, d, lo, hi)

    def z_outward(arrays):
        z_right(arrays, nk - 2)
        z_left(arrays, 1)

    def y_own(a):
        for q in range(pieces(a)):
            y_copy(a, k, q).start()

    def relay(a, of_k, q):
        f_wait(a, 2 * of_k + p, q)
        y_copy(a, of_k, q).start()

    def relay_all(a, of_k):
        for q in range(pieces(a)):
            relay(a, of_k, q)

    def f_drain(a):
        for kk in range(nk):
            for q in range(pieces(a)):
                y_copy(a, kk, q).wait_send()

            @pl.when(k != kk)
            def _(kk=kk):
                for q in range(pieces(a)):
                    z_copy(a, kk, q).wait_send()

    group = k // 2
    order = [2 * group, 2 * group + 1]
    for m in range(1, nk // 2):
        low = (group // (1 << (m.bit_length() - 1))) % 2
        for j in (0, 1):
            order.append(2 * xor(group, m) + low * (1 - j) + (1 - low) * j)
    later = [(of_k, q) for of_k in order[2:] for q in range(n_pc)]

    def relay_some(a, lo, hi):
        for of_k, q in later[lo:hi]:
            relay(a, of_k, q)

    def partners_wait(a):
        for of_k in order:
            for q in range(pieces(a)):
                f_wait(a, 2 * of_k + 1 - p, q)

    def at_inner(fn):
        pl.when(inner)(fn)

    def at_end(fn):
        pl.when(jnp.logical_not(inner))(fn)

    starts = [0]
    for b in range(bits):
        starts.append(starts[-1] + ((t // (1 << b)) % 2) * (seq >> (b + 1)))

    def aways(b):
        return starts[b] + (1 - (t // (1 << b)) % 2) * (seq >> (b + 1))

    n_t = [0]

    def t_copy(src, dst, device):
        i = n_t[0]
        n_t[0] += 1
        return remote(src, dst, t_send.at[i], t_recv.at[i], device)

    def landing(b):
        return seq - (seq >> b)

    class Split:
        def __init__(self, n, make):
            self.parts = [make(n // hops * h, n // hops) for h in range(hops)]

        def start(self):
            for c in self.parts:
                c.start()

        def wait_recv(self):
            for c in self.parts:
                c.wait_recv()

        def wait_send(self):
            for c in self.parts:
                c.wait_send()

    def shift(start, lo, n):
        return pl.ds(pl.multiple_of(start + lo, n), n)

    def reduce_copy(i, b):
        return Split(
            seq >> (b + 1),
            lambda lo, n: t_copy(
                part.at[i, shift(aways(b), lo, n)],
                recv.at[i, pl.ds(landing(b) + lo, n)],
                {"tp": flip(1 << b)},
            ),
        )

    def add_recv(i, b, start, n, origin=None):
        base = landing(b) - (starts[b + 1] if origin is None else origin)
        tile = min(n, 64)

        @pl.loop(0, n // tile)
        def _(j):
            mine = pl.ds(pl.multiple_of(start + j * tile, tile), tile)
            theirs = pl.ds(pl.multiple_of(base + start + j * tile, tile), tile)
            part[i, mine] = (part[i, mine].astype(f32) + recv[i, theirs].astype(f32)).astype(bf16)

    last = bits - 1
    n_own = seq >> bits
    own_rows = span(starts[bits], n_own)

    tok_z = t_copy(tokens.at[own_rows], tok_m.at[own_rows], {"fs": mate})
    tok_g = []
    for b in range(bits):
        ref = tok_m.at[span(starts[b + 1], seq >> (b + 1))]
        tok_g.append(t_copy(ref, ref, {"tp": flip(1 << b)}))
    reduces = [[reduce_copy(i, b) for b in range(bits)] for i in (0, 1)]
    sum_z = Split(
        n_own,
        lambda lo, n: t_copy(
            part.at[1, shift(starts[bits], lo, n)], r_sum.at[pl.ds(lo, n)], {"fs": mate}
        ),
    )

    def mate_piece(lo, n):
        ref = first.at[e, shift(starts[bits], lo, n)]
        return t_copy(ref, ref, {"fs": mate})

    to_mate = Split(n_own, mate_piece)
    gathers = []
    for i in (e, 1 - e):
        gathers.append([])
        for b in range(bits):


            def gather_piece(lo, n):
                ref = first.at[i, shift(starts[b + 1], lo, n)]
                return t_copy(ref, ref, {"tp": flip(1 << b)})

            gathers[-1].append(Split(seq >> (b + 1), gather_piece))
    own_g, mate_g = gathers

    ins = (0, 1, 2)
    tok_z.start()
    z_all(ins)
    z_all((3,))
    z_all((UP,))
    for c in copies:
        c.wait()
    for a in range(UP + 1):
        y_own(a)
    tok_z.wait_recv()
    tok_g[last].start()
    for of_k in [mate_k] + order[2:3]:
        for a in ins:
            relay(a, of_k, 0)
    for b in range(last, 0, -1):
        tok_g[b].wait_recv()
        tok_g[b - 1].start()
    for of_k in order[3:]:
        for a in ins:
            relay(a, of_k, 0)
    for of_k in [mate_k] + order[2:]:
        relay(3, of_k, 0)
    tok_g[0].wait_recv()
    for a in ins:
        partners_wait(a)

    @at_inner
    def _():
        relay_all(UP, mate_k)

    at_end(lambda: y_own(DN))

    pad = zpad.shape[1] - seq
    n_taps = taps.shape[0]
    tile = min(256, seq)

    def project(i, x_ref):
        zpad[i, 0:pad] = jnp.zeros((pad, hc), f32)

        @pl.loop(0, seq // tile)
        def _(j):
            at = pl.ds(pl.multiple_of(j * tile, tile), tile)
            x = x_ref[at]
            if hc % 128 == 0:
                w = jnp.concatenate([mix_g[a] for a in ins], axis=1)
                y = jnp.dot(x, w, preferred_element_type=f32)
                ys = [y[:, a * hc : (a + 1) * hc] for a in ins]
            else:
                ys = [jnp.dot(x, mix_g[a], preferred_element_type=f32) for a in ins]
            outer[i, at] = ys[0]
            zpad[i, pl.ds(pl.multiple_of(j * tile + pad, 8), tile)] = ys[1] * ys[2]

        acc = jnp.zeros((seq, hc), f32)
        for j in range(n_taps):
            lo = pad - (n_taps - 1) + j
            acc = acc + tap_rows[j : j + 1] * zpad[i, lo : lo + seq]
        conv[i] = (outer[i] * acc).astype(bf16)

    if len(taps.shape) == 3:
        tap_rows = taps[:, e, :]
    else:
        tap_rows = taps[:, span(e * hc, hc)]
    wide = min(256, width)

    def mix_out(i, start):
        at_rows = span(start, hs)
        lhs = conv[i, at_rows]

        @pl.loop(0, width // wide)
        def _(j):
            at = pl.ds(pl.multiple_of(j * wide, wide), wide)
            part[i, at_rows, at] = lax.dot_general(
                lhs, mix_g[3, at], NT, preferred_element_type=f32
            ).astype(bf16)

    def stage_up(i, b):
        n = seq >> (b + 1)
        reduces[i][b - 1].wait_recv()
        add_recv(i, b - 1, aways(b), n)
        reduces[i][b].start()
        add_recv(i, b - 1, starts[b + 1], n)

    for i, x_ref in ((1, tok_m), (0, tokens)):
        project(i, x_ref)
        if i:
            partners_wait(3)
        mix_out(i, aways(0))
        reduces[i][0].start()
        mix_out(i, starts[1])
        stage_up(i, 1)
    for b in range(2, bits):
        for i in (1, 0):
            stage_up(i, b)

    n_l = len(later)
    early = n_pc // 2

    @at_end
    def _():
        relay_all(UP, mate_k)

    at_inner(lambda: relay_some(UP, 0, n_pc))
    for h in range(hops):
        n_h = n_own // hops
        reduces[1][last].parts[h].wait_recv()
        add_recv(1, last, starts[bits] + h * n_h, n_h, starts[bits])
        sum_z.parts[h].start()
    z_mid((DN,), 1, 2)
    at_end(lambda: relay_some(UP, 0, n_pc))
    relay_some(UP, n_pc, n_l)
    at_inner(lambda: y_own(DN))
    reduces[0][last].wait_recv()
    sum_z.wait_recv()
    tile_n = min(n_own, 64)

    @pl.loop(0, n_own // tile_n)
    def _(i):
        at = pl.ds(pl.multiple_of(starts[bits] + i * tile_n, tile_n), tile_n)
        here = pl.ds(pl.multiple_of(i * tile_n, tile_n), tile_n)
        theirs = pl.ds(pl.multiple_of(landing(last) + i * tile_n, tile_n), tile_n)
        total = part[0, at].astype(f32) + recv[0, theirs].astype(f32) + r_sum[here].astype(f32)
        first[e, at] = layer_norm(
            residual_scale * tokens[at].astype(f32) + total, m_gain[...], m_shift[...]
        ).astype(bf16)

    to_mate.start()
    own_g[last].start()
    z_ends((DN,), 1)
    z_outward((DN,))
    z_mid((DN,), 2)
    for b in range(last, 0, -1):
        own_g[b].wait_recv()
        own_g[b - 1].start()
    wide_u = min(256, half)

    def up(q):
        @pl.loop(0, half // wide_u)
        def _(i):
            at = pl.ds(pl.multiple_of(i * wide_u, wide_u), wide_u)
            u = jnp.maximum(jnp.dot(first[q], up_g[:, at], preferred_element_type=f32), 0.0)
            hidden[q, :, at] = (u * u).astype(bf16)

    @at_inner
    def _():
        for h in range(hops):
            to_mate.parts[h].wait_recv()
            mate_g[last].parts[h].start()

    at_inner(lambda: relay_some(DN, 0, n_pc))
    own_g[0].wait_recv()
    partners_wait(UP)
    up(e)

    @at_end
    def _():
        for h in range(hops):
            to_mate.parts[h].wait_recv()
            mate_g[last].parts[h].start()

    at_end(lambda: relay_some(DN, 0, n_pc))
    for q in range(early):
        relay(DN, mate_k, q)
    for b in range(last, 0, -1):
        mate_g[b].wait_recv()
        mate_g[b - 1].start()
    for q in range(early, n_pc):
        relay(DN, mate_k, q)
    mate_g[0].wait_recv()
    up(1 - e)

    cw = 2 * rows // sub
    mine_h = pl.ds(pl.multiple_of(core * hs, hs), hs)
    away_h = pl.ds(pl.multiple_of((1 - core) * hs, hs), hs)
    chunks = []
    for of_k in order[2:3] + order[:2] + order[3:]:
        for i in range(sub):
            side = (p, 1 - p)[i] if sub == 2 else 0
            chunks.append((of_k, (2 * of_k + side) * rows, i))

    def cols_of(j):
        return pl.ds(pl.multiple_of(chunks[j][1], cw), cw)

    def s1(j):
        c = cols_of(j)
        return remote(
            part2.at[:, away_h, c],
            r_core.at[:, :, c],
            s1_send.at[j],
            s1_recv.at[j],
            {"tp": flip(1)},
        )

    def s2(j):
        c = cols_of(j)
        return remote(
            part2.at[1 - e, mine_h, c],
            r_mate.at[:, c],
            s2_send.at[j],
            s2_recv.at[j],
            {"fs": mate},
        )

    def s3(j, b):
        c = cols_of(j)
        return remote(
            part2.at[e, mine_h, c],
            r_x.at[b - 1, :, c],
            s3_send.at[b - 1, j],
            s3_recv.at[b - 1, j],
            {"tp": flip(1 << b)},
        )

    def product(j):
        c = cols_of(j)
        w = dn_g[c]

        @pl.loop(0, 2)
        def _(q):
            part2[q, :, c] = lax.dot_general(
                hidden[q], w, NT, preferred_element_type=f32
            ).astype(bf16)

        s1(j).start()

    def core_sum(j):
        c = cols_of(j)
        s1(j).wait_recv()
        part2[1 - e, mine_h, c] = (
            part2[1 - e, mine_h, c].astype(f32) + r_core[1 - e, :, c].astype(f32)
        ).astype(bf16)
        s2(j).start()

    def mate_sum(j):
        c = cols_of(j)
        s2(j).wait_recv()
        part2[e, mine_h, c] = (
            part2[e, mine_h, c].astype(f32)
            + r_core[e, :, c].astype(f32)
            + r_mate[:, c].astype(f32)
        ).astype(bf16)
        s3(j, 1).start()

    def x_sum(j, b):
        c = cols_of(j)
        s3(j, b - 1).wait()
        part2[e, mine_h, c] = (
            part2[e, mine_h, c].astype(f32) + r_x[b - 2, :, c].astype(f32)
        ).astype(bf16)
        s3(j, b).start()

    stages = [core_sum, mate_sum]
    for b in range(2, bits):
        stages.append(functools.partial(x_sum, b=b))
    n_ch = len(chunks)

    def later_sums(j):
        for i, stage in enumerate(stages[1:]):
            if 0 <= j - i < n_ch:
                stage(j - i)

    def chunk(j):
        if j % sub == sub - 1:
            for q in range(n_pc):
                f_wait(DN, 2 * chunks[j][0] + 1 - p, q)
        product(j)
        if j >= 1:
            core_sum(j - 1)

    summed = 0
    n_first = 3 * sub
    for j in range(n_first):
        chunk(j)
    for m in range(1, n_l // n_pc):
        ready = (m + 2) * sub - 1
        for q in range(n_pc):
            if summed < ready:
                later_sums(summed)
                summed += 1
            relay_some(DN, m * n_pc + q, m * n_pc + q + 1)
        for j in range((m + 2) * sub, (m + 3) * sub):
            chunk(j)
            if summed < j - 1:
                later_sums(summed)
                summed += 1
    core_sum(n_ch - 1)
    for j in range(summed, n_ch + len(stages) - 2):
        later_sums(j)

    n_out = o_send.shape[0]
    piece_rows = hs // n_out
    tile_o = min(piece_rows, 64)

    def out_rows(i):
        return pl.ds(pl.multiple_of(core * hs + i * piece_rows, piece_rows), piece_rows)

    def out_local(i):
        return pltpu.make_async_copy(
            result.at[pl.ds(i * piece_rows, piece_rows)], out.at[out_rows(i)], out_sem.at[i]
        )

    def out_remote(i):
        return remote(
            result.at[pl.ds(i * piece_rows, piece_rows)],
            out.at[out_rows(i)],
            o_send.at[i],
            o_recv.at[i],
            {"tp": flip(1)},
        )

    for j in range(n_ch):
        s3(j, last).wait_recv()
    for i in range(n_out):

        @pl.loop(0, piece_rows // tile_o)
        def _(ii):
            lo = i * piece_rows + ii * tile_o
            here = pl.ds(pl.multiple_of(lo, tile_o), tile_o)
            at = pl.ds(pl.multiple_of(core * hs + lo, tile_o), tile_o)
            total = part2[e, at].astype(f32) + r_x[last - 1, here].astype(f32)
            result[here] = layer_norm(
                residual_scale * first[e, at].astype(f32) + total, c_gain[...], c_shift[...]
            ).astype(bf16)

        out_local(i).start()
        out_remote(i).start()

    for a in range(6):
        f_drain(a)
    for c in [tok_z, sum_z, to_mate] + tok_g + reduces[0] + reduces[1] + own_g + mate_g:
        c.wait_send()
    for j in range(n_ch):
        s1(j).wait_send()
        s2(j).wait_send()
        s3(j, last).wait_send()
    for i in range(n_out):
        out_local(i).wait()
        out_remote(i).wait()


def local(
    tokens,
    gate_outer,
    gate_inner,
    conv_input,
    mixer_output,
    conv_taps,
    mixer_gain,
    mixer_shift,
    up_weight,
    down_weight,
    channel_gain,
    channel_shift,
):
    seq, width = tokens.shape
    rows, units = up_weight.shape
    chans = gate_outer.shape[1]
    half = units // 2
    n_fs = lax.axis_size("fs")
    n_tp = lax.axis_size("tp")
    bits = n_tp.bit_length() - 1
    nk = n_fs // 2
    hc = chans // 2
    sub = 2 if rows % 128 == 0 else 1
    n_ch = nk * sub
    hs = seq // 2
    n_out = 4
    n_pc = min(4, rows // 16)
    hops = 2
    n_t = bits + 1 + hops * (4 * bits + 2)
    mix = (gate_outer, gate_inner, conv_input, mixer_output)
    if hc % 128:
        mix = tuple(w.reshape(rows, 2, hc).swapaxes(0, 1) for w in mix)
        conv_taps = conv_taps.reshape(-1, 2, hc)
    vmem = pl.BlockSpec(memory_space=pltpu.VMEM)
    dma = pltpu.SemaphoreType.DMA
    return pl.pallas_call(
        functools.partial(kernel, n_fs, n_tp, sub, n_pc, hops),
        out_shape=jax.ShapeDtypeStruct((seq, width), bf16),
        in_specs=[vmem] * 12,
        out_specs=pl.BlockSpec(memory_space=pl.ANY),
        scratch_shapes=[
            pltpu.VMEM((4, width, hc), bf16),
            pltpu.VMEM((width, half), bf16),
            pltpu.VMEM((width, half), bf16),
            pltpu.VMEM((seq, width), bf16),
            pltpu.VMEM((2, seq, hc), f32),
            pltpu.VMEM((2, seq + 8, hc), f32),
            pltpu.VMEM((2, seq, hc), bf16),
            pltpu.VMEM((2, seq, width), bf16),
            pltpu.VMEM((2, seq, width), bf16),
            pltpu.VMEM((seq // n_tp, width), bf16),
            pltpu.VMEM((2, seq, width), bf16),
            pltpu.VMEM((2, seq, half), bf16),
            pltpu.VMEM((2, seq, width), bf16),
            pltpu.VMEM((2, hs, width), bf16),
            pltpu.VMEM((hs, width), bf16),
            pltpu.VMEM((bits - 1, hs, width), bf16),
            pltpu.VMEM((hs, width), bf16),
            dma((6, n_pc)),
            dma((n_out,)),
            dma((6, nk, n_pc)),
            dma((6, nk, n_pc)),
            dma((6, n_fs, n_pc)),
            dma((n_t,)),
            dma((n_t,)),
            dma((n_ch,)),
            dma((n_ch,)),
            dma((n_ch,)),
            dma((n_ch,)),
            dma((bits - 1, n_ch)),
            dma((bits - 1, n_ch)),
            dma((n_out,)),
            dma((n_out,)),
        ],
        compiler_params=pltpu.CompilerParams(
            collective_id=0, has_side_effects=True, vmem_limit_bytes=62 * 1024 * 1024
        ),
    )(
        tokens,
        *mix,
        conv_taps,
        mixer_gain.reshape(1, width),
        mixer_shift.reshape(1, width),
        up_weight,
        down_weight,
        channel_gain.reshape(1, width),
        channel_shift.reshape(1, width),
    )


def solution(mesh):
    in_specs = (
        P(("rep", "fs"), None),
        P("fs", "tp"),
        P("fs", "tp"),
        P("fs", "tp"),
        P("fs", "tp"),
        P(None, "tp"),
        P(),
        P(),
        P("fs", "tp"),
        P("fs", "tp"),
        P(),
        P(),
    )
    out_specs = P(("rep", "fs"), None)
    return jax.shard_map(local, mesh=mesh, in_specs=in_specs, out_specs=out_specs, check_vma=False)
```

```python
import functools

import jax
import jax.numpy as jnp
from jax import lax
from jax.experimental import pallas as pl
from jax.experimental.pallas import tpu as pltpu
from jax.sharding import PartitionSpec as P

residual_scale = 8.0**0.25
norm_epsilon = 1e-05
MESH = pl.DeviceIdType.MESH
f32 = jnp.float32
bf16 = jnp.bfloat16
NT = (((1,), (1,)), ((), ()))


def layer_norm(values, gain, shift):
    row_mean = jnp.mean(values, -1, keepdims=True)
    centered = values - row_mean
    variance = jnp.mean(centered * centered, -1, keepdims=True)
    return centered * lax.rsqrt(variance + norm_epsilon) * gain + shift


def xor(value, mask):
    bit = 1
    while bit <= mask:
        if mask & bit:
            value = value + bit - 2 * bit * ((value // bit) % 2)
        bit *= 2
    return value


def kernel(
    n_fs,
    n_tp,
    sub,
    n_pc,
    hops,
    tokens_in,
    w_go,
    w_gi,
    w_ci,
    w_mo,
    taps_in,
    m_gain_in,
    m_shift_in,
    w_up,
    w_dn,
    c_gain_in,
    c_shift_in,
    out,
    tokens,
    taps,
    m_gain,
    m_shift,
    c_gain,
    c_shift,
    mix_g,
    up_g,
    dn_g,
    tok_m,
    outer,
    zpad,
    conv,
    part,
    recv,
    r_sum,
    first,
    hidden,
    part2,
    r_core,
    r_mate,
    r_x,
    r_half,
    local_sem,
    in_sem,
    z_sends,
    y_sends,
    f_recv,
    t_send,
    t_recv,
    s1_send,
    s1_recv,
    s2_send,
    s2_recv,
    s3_send,
    s3_recv,
    h_send,
    h_recv,
    o_send,
    o_recv,
):
    seq, width = tokens.shape
    rows = w_up.shape[0]
    half = w_up.shape[1] // 2
    hc = mix_g.shape[2]
    bits = n_tp.bit_length() - 1
    nk = n_fs // 2
    f = lax.axis_index("fs")
    t = lax.axis_index("tp")
    k = f // 2
    p = f % 2
    partner = f + 1 - 2 * p
    e = k % 2
    mate_k = k + 1 - 2 * e
    mate = 2 * mate_k + p
    core = t % 2
    hs = seq // 2
    inner = jnp.logical_and(k > 0, k < nk - 1)

    def flip(bit):
        return t + bit - 2 * bit * ((t // bit) % 2)

    def span(start, n):
        return pl.ds(pl.multiple_of(start, n), n)

    def remote(src, dst, ssem, rsem, device):
        return pltpu.make_async_remote_copy(
            src_ref=src,
            dst_ref=dst,
            send_sem=ssem,
            recv_sem=rsem,
            device_id=device,
            device_id_type=MESH,
        )

    sources = (w_go, w_gi, w_ci, w_mo, w_up, w_dn)
    UP, DN = 4, 5

    def pieces(a):
        return n_pc if a >= UP else 1

    def source(a, parity, q):
        w = sources[a]
        pn = rows // pieces(a)
        at = pl.ds(q * pn, pn)
        if len(w.shape) == 3:
            return w.at[parity, at]
        n = half if a >= UP else hc
        return w.at[at, span(parity * n, n)]

    def held(a, s, q):
        pn = rows // pieces(a)
        at = span(s * rows + q * pn, pn)
        if a < UP:
            return mix_g.at[a, at]
        return (up_g if a == UP else dn_g).at[at]

    copies = []
    for a in range(6):
        for q in range(pieces(a)):
            copies.append(
                pltpu.make_async_copy(source(a, e, q), held(a, f, q), local_sem.at[a, q])
            )
    small = (
        (tokens_in, tokens),
        (taps_in, taps),
        (m_gain_in, m_gain),
        (m_shift_in, m_shift),
        (c_gain_in, c_gain),
        (c_shift_in, c_shift),
    )
    for i, (here, there) in enumerate(small):
        copies.append(pltpu.make_async_copy(here, there, in_sem.at[i]))
    barrier = pltpu.get_barrier_semaphore()
    pl.semaphore_signal(barrier, inc=1, device_id={"fs": partner}, device_id_type=MESH)
    for i in range(1, nk):
        pl.semaphore_signal(
            barrier, inc=1, device_id={"fs": 2 * xor(k, i) + p}, device_id_type=MESH
        )
    for b in range(bits):
        pl.semaphore_signal(barrier, inc=1, device_id={"tp": flip(1 << b)}, device_id_type=MESH)
    for c in copies:
        c.start()
    pl.semaphore_wait(barrier, nk + bits)

    def z_copy(a, to_k, q):
        return remote(
            source(a, to_k % 2, q),
            held(a, f, q),
            z_sends.at[a, to_k, q],
            f_recv.at[a, f, q],
            {"fs": 2 * to_k + p},
        )

    def y_copy(a, of_k, q):
        ref = held(a, 2 * of_k + p, q)
        return remote(
            ref, ref, y_sends.at[a, of_k, q], f_recv.at[a, 2 * of_k + p, q], {"fs": partner}
        )

    def f_wait(a, s, q):
        ref = held(a, s, q)
        remote(ref, ref, y_sends.at[a, 0, q], f_recv.at[a, s, q], {"fs": partner}).wait_recv()

    def z_send(a, kk):
        for q in range(pieces(a)):
            z_copy(a, kk, q).start()

    def z_right(arrays, d, lo=1, hi=None):
        @pl.when(k == d)
        def _():
            for kk in range(d + lo, nk if hi is None else min(d + hi, nk)):
                for a in arrays:
                    z_send(a, kk)

    def z_left(arrays, d, lo=1, hi=None):
        @pl.when(k == d)
        def _():
            for kk in range(d - lo, -1 if hi is None else max(d - hi, -1), -1):
                for a in arrays:
                    z_send(a, kk)

    def z_all(arrays):
        for d in range(nk):
            z_right(arrays, d)
            z_left(arrays, d)

    def z_ends(arrays, lo, hi=None):
        z_right(arrays, 0, lo, hi)
        z_left(arrays, nk - 1, lo, hi)

    def z_mid(arrays, lo=1, hi=None):
        for d in range(1, nk - 1):
            if d < nk - 2:
                z_right(arrays, d, lo, hi)
            if d > 1:
                z_left(arrays, d, lo, hi)

    def z_outward(arrays):
        z_right(arrays, nk - 2)
        z_left(arrays, 1)

    def y_own(a):
        for q in range(pieces(a)):
            y_copy(a, k, q).start()

    def relay(a, of_k, q):
        f_wait(a, 2 * of_k + p, q)
        y_copy(a, of_k, q).start()

    def relay_all(a, of_k):
        for q in range(pieces(a)):
            relay(a, of_k, q)

    def f_drain(a):
        for kk in range(nk):
            for q in range(pieces(a)):
                y_copy(a, kk, q).wait_send()

            @pl.when(k != kk)
            def _(kk=kk):
                for q in range(pieces(a)):
                    z_copy(a, kk, q).wait_send()

    group = k // 2
    order = [2 * group, 2 * group + 1]
    for m in range(1, nk // 2):
        low = (group // (1 << (m.bit_length() - 1))) % 2
        for j in (0, 1):
            order.append(2 * xor(group, m) + low * (1 - j) + (1 - low) * j)
    later = [(of_k, q) for of_k in order[2:] for q in range(n_pc)]

    def relay_some(a, lo, hi):
        for of_k, q in later[lo:hi]:
            relay(a, of_k, q)

    def partners_wait(a):
        for of_k in order:
            for q in range(pieces(a)):
                f_wait(a, 2 * of_k + 1 - p, q)

    def at_inner(fn):
        pl.when(inner)(fn)

    def at_end(fn):
        pl.when(jnp.logical_not(inner))(fn)

    starts = [0]
    for b in range(bits):
        starts.append(starts[-1] + ((t // (1 << b)) % 2) * (seq >> (b + 1)))

    def aways(b):
        return starts[b] + (1 - (t // (1 << b)) % 2) * (seq >> (b + 1))

    n_t = [0]

    def t_copy(src, dst, device):
        i = n_t[0]
        n_t[0] += 1
        return remote(src, dst, t_send.at[i], t_recv.at[i], device)

    def landing(b):
        return seq - (seq >> b)

    class Split:
        def __init__(self, n, make):
            self.parts = [make(n // hops * h, n // hops) for h in range(hops)]

        def start(self):
            for c in self.parts:
                c.start()

        def wait_recv(self):
            for c in self.parts:
                c.wait_recv()

        def wait_send(self):
            for c in self.parts:
                c.wait_send()

    def shift(start, lo, n):
        return pl.ds(pl.multiple_of(start + lo, n), n)

    def reduce_copy(i, b):
        return Split(
            seq >> (b + 1),
            lambda lo, n: t_copy(
                part.at[i, shift(aways(b), lo, n)],
                recv.at[i, pl.ds(landing(b) + lo, n)],
                {"tp": flip(1 << b)},
            ),
        )

    def add_recv(i, b, start, n, origin=None):
        base = landing(b) - (starts[b + 1] if origin is None else origin)
        tile = min(n, 64)

        @pl.loop(0, n // tile)
        def _(j):
            mine = pl.ds(pl.multiple_of(start + j * tile, tile), tile)
            theirs = pl.ds(pl.multiple_of(base + start + j * tile, tile), tile)
            part[i, mine] = (part[i, mine].astype(f32) + recv[i, theirs].astype(f32)).astype(bf16)

    last = bits - 1
    n_own = seq >> bits
    own_rows = span(starts[bits], n_own)

    tok_z = t_copy(tokens_in.at[own_rows], tok_m.at[own_rows], {"fs": mate})
    tok_g = []
    for b in range(bits):
        ref = tok_m.at[span(starts[b + 1], seq >> (b + 1))]
        tok_g.append(t_copy(ref, ref, {"tp": flip(1 << b)}))
    reduces = [[reduce_copy(i, b) for b in range(bits)] for i in (0, 1)]
    sum_z = Split(
        n_own,
        lambda lo, n: t_copy(
            part.at[1, shift(starts[bits], lo, n)], r_sum.at[pl.ds(lo, n)], {"fs": mate}
        ),
    )

    def mate_piece(lo, n):
        ref = first.at[e, shift(starts[bits], lo, n)]
        return t_copy(ref, ref, {"fs": mate})

    to_mate = Split(n_own, mate_piece)
    gathers = []
    for i in (e, 1 - e):
        gathers.append([])
        for b in range(bits):


            def gather_piece(lo, n):
                ref = first.at[i, shift(starts[b + 1], lo, n)]
                return t_copy(ref, ref, {"tp": flip(1 << b)})

            gathers[-1].append(Split(seq >> (b + 1), gather_piece))
    own_g, mate_g = gathers

    ins = (0, 1, 2)
    tok_z.start()
    z_all(ins)
    z_all((3,))
    z_all((UP,))
    for c in copies:
        c.wait()
    for a in range(UP + 1):
        y_own(a)
    tok_z.wait_recv()
    tok_g[last].start()
    for of_k in [mate_k] + order[2:3]:
        for a in ins:
            relay(a, of_k, 0)
    for b in range(last, 0, -1):
        tok_g[b].wait_recv()
        tok_g[b - 1].start()
    for of_k in order[3:]:
        for a in ins:
            relay(a, of_k, 0)
    for of_k in [mate_k] + order[2:]:
        relay(3, of_k, 0)
    tok_g[0].wait_recv()
    for a in ins:
        partners_wait(a)

    @at_inner
    def _():
        relay_all(UP, mate_k)

    at_end(lambda: y_own(DN))

    pad = zpad.shape[1] - seq
    n_taps = taps.shape[0]
    tile = min(256, seq)

    def project(i, x_ref):
        zpad[i, 0:pad] = jnp.zeros((pad, hc), f32)

        @pl.loop(0, seq // tile)
        def _(j):
            at = pl.ds(pl.multiple_of(j * tile, tile), tile)
            x = x_ref[at]
            if hc % 128 == 0:
                w = jnp.concatenate([mix_g[a] for a in ins], axis=1)
                y = jnp.dot(x, w, preferred_element_type=f32)
                ys = [y[:, a * hc : (a + 1) * hc] for a in ins]
            else:
                ys = [jnp.dot(x, mix_g[a], preferred_element_type=f32) for a in ins]
            outer[i, at] = ys[0]
            zpad[i, pl.ds(pl.multiple_of(j * tile + pad, 8), tile)] = ys[1] * ys[2]

        acc = jnp.zeros((seq, hc), f32)
        for j in range(n_taps):
            lo = pad - (n_taps - 1) + j
            acc = acc + tap_rows[j : j + 1] * zpad[i, lo : lo + seq]
        conv[i] = (outer[i] * acc).astype(bf16)

    if len(taps.shape) == 3:
        tap_rows = taps[:, e, :]
    else:
        tap_rows = taps[:, span(e * hc, hc)]
    wide = min(256, width)

    def mix_out(i, start):
        at_rows = span(start, hs)
        lhs = conv[i, at_rows]

        @pl.loop(0, width // wide)
        def _(j):
            at = pl.ds(pl.multiple_of(j * wide, wide), wide)
            part[i, at_rows, at] = lax.dot_general(
                lhs, mix_g[3, at], NT, preferred_element_type=f32
            ).astype(bf16)

    def stage_up(i, b):
        n = seq >> (b + 1)
        reduces[i][b - 1].wait_recv()
        add_recv(i, b - 1, aways(b), n)
        reduces[i][b].start()
        add_recv(i, b - 1, starts[b + 1], n)

    for i, x_ref in ((1, tok_m), (0, tokens)):
        project(i, x_ref)
        if i:
            partners_wait(3)
        mix_out(i, aways(0))
        reduces[i][0].start()
        mix_out(i, starts[1])
        stage_up(i, 1)
    for b in range(2, bits):
        for i in (1, 0):
            stage_up(i, b)

    n_l = len(later)
    early = n_pc // 2

    @at_end
    def _():
        relay_all(UP, mate_k)

    at_inner(lambda: relay_some(UP, 0, n_pc))
    for h in range(hops):
        n_h = n_own // hops
        reduces[1][last].parts[h].wait_recv()
        add_recv(1, last, starts[bits] + h * n_h, n_h, starts[bits])
        sum_z.parts[h].start()
    z_mid((DN,), 1, 2)
    at_end(lambda: relay_some(UP, 0, n_pc))
    relay_some(UP, n_pc, n_l)
    at_inner(lambda: y_own(DN))
    reduces[0][last].wait_recv()
    sum_z.wait_recv()
    tile_n = min(n_own, 64)

    @pl.loop(0, n_own // tile_n)
    def _(i):
        at = pl.ds(pl.multiple_of(starts[bits] + i * tile_n, tile_n), tile_n)
        here = pl.ds(pl.multiple_of(i * tile_n, tile_n), tile_n)
        theirs = pl.ds(pl.multiple_of(landing(last) + i * tile_n, tile_n), tile_n)
        total = part[0, at].astype(f32) + recv[0, theirs].astype(f32) + r_sum[here].astype(f32)
        first[e, at] = layer_norm(
            residual_scale * tokens[at].astype(f32) + total, m_gain[...], m_shift[...]
        ).astype(bf16)

    to_mate.start()
    own_g[last].start()
    z_ends((DN,), 1)
    z_outward((DN,))
    z_mid((DN,), 2)
    for b in range(last, 0, -1):
        own_g[b].wait_recv()
        own_g[b - 1].start()
    wide_u = min(256, half)

    def up(q):
        @pl.loop(0, half // wide_u)
        def _(i):
            at = pl.ds(pl.multiple_of(i * wide_u, wide_u), wide_u)
            u = jnp.maximum(jnp.dot(first[q], up_g[:, at], preferred_element_type=f32), 0.0)
            hidden[q, :, at] = (u * u).astype(bf16)

    @at_inner
    def _():
        for h in range(hops):
            to_mate.parts[h].wait_recv()
            mate_g[last].parts[h].start()

    at_inner(lambda: relay_some(DN, 0, n_pc))
    own_g[0].wait_recv()
    partners_wait(UP)
    up(e)

    @at_end
    def _():
        for h in range(hops):
            to_mate.parts[h].wait_recv()
            mate_g[last].parts[h].start()

    at_end(lambda: relay_some(DN, 0, n_pc))
    for q in range(early):
        relay(DN, mate_k, q)
    for b in range(last, 0, -1):
        mate_g[b].wait_recv()
        mate_g[b - 1].start()
    for q in range(early, n_pc):
        relay(DN, mate_k, q)
    mate_g[0].wait_recv()
    up(1 - e)

    cw = 2 * rows // sub
    mine_h = pl.ds(pl.multiple_of(core * hs, hs), hs)
    away_h = pl.ds(pl.multiple_of((1 - core) * hs, hs), hs)
    chunks = []
    for of_k in order[2:3] + order[:2] + order[3:]:
        for i in range(sub):
            side = (p, 1 - p)[i] if sub == 2 else 0
            chunks.append((of_k, (2 * of_k + side) * rows, i))

    def cols_of(j):
        return pl.ds(pl.multiple_of(chunks[j][1], cw), cw)

    def s1(j):
        c = cols_of(j)
        return remote(
            part2.at[:, away_h, c],
            r_core.at[:, :, c],
            s1_send.at[j],
            s1_recv.at[j],
            {"tp": flip(1)},
        )

    def s2(j):
        c = cols_of(j)
        return remote(
            part2.at[1 - e, mine_h, c],
            r_mate.at[:, c],
            s2_send.at[j],
            s2_recv.at[j],
            {"fs": mate},
        )

    def s3(j, b):
        c = cols_of(j)
        return remote(
            part2.at[e, mine_h, c],
            r_x.at[b - 1, :, c],
            s3_send.at[b - 1, j],
            s3_recv.at[b - 1, j],
            {"tp": flip(1 << b)},
        )

    def product(j):
        c = cols_of(j)
        w = dn_g[c]

        @pl.loop(0, 2)
        def _(q):
            part2[q, :, c] = lax.dot_general(
                hidden[q], w, NT, preferred_element_type=f32
            ).astype(bf16)

        s1(j).start()

    def core_sum(j):
        if j < n_half:
            half_core(j)
            return
        c = cols_of(j)
        s1(j).wait_recv()
        part2[1 - e, mine_h, c] = (
            part2[1 - e, mine_h, c].astype(f32) + r_core[1 - e, :, c].astype(f32)
        ).astype(bf16)
        s2(j).start()

    quarter = hs // 2
    bit = (t // 2) % 2
    own_q = shift(core * hs + bit * quarter, 0, quarter)
    away_q = shift(core * hs + (1 - bit) * quarter, 0, quarter)
    own_r = shift(bit * quarter, 0, quarter)
    away_r = shift((1 - bit) * quarter, 0, quarter)

    def h1(j):
        c = cols_of(j)
        return remote(
            part2.at[1 - e, away_q, c],
            r_half.at[:, c],
            h_send.at[0, j],
            h_recv.at[0, j],
            {"tp": flip(2)},
        )

    def h2(j):
        c = cols_of(j)
        return remote(
            part2.at[e, away_q, c],
            r_x.at[0, away_r, c],
            h_send.at[1, j],
            h_recv.at[1, j],
            {"tp": flip(2)},
        )

    def h2_wait(j):
        c = cols_of(j)
        remote(
            part2.at[e, own_q, c],
            r_x.at[0, own_r, c],
            h_send.at[1, j],
            h_recv.at[1, j],
            {"tp": flip(2)},
        ).wait_recv()

    def h3(j):
        c = cols_of(j)
        return remote(
            part2.at[1 - e, own_q, c],
            r_mate.at[own_r, c],
            s2_send.at[j],
            s2_recv.at[j],
            {"fs": mate},
        )

    def h4(j):
        c = cols_of(j)
        return remote(
            part2.at[e, own_q, c],
            r_x.at[0, own_r, c],
            s3_send.at[0, j],
            s3_recv.at[0, j],
            {"tp": flip(2)},
        )

    def h4_wait(j):
        c = cols_of(j)
        remote(
            part2.at[e, away_q, c],
            r_x.at[0, away_r, c],
            s3_send.at[0, j],
            s3_recv.at[0, j],
            {"tp": flip(2)},
        ).wait_recv()

    def plus(i, at, c, other):
        part2[i, at, c] = (part2[i, at, c].astype(f32) + other.astype(f32)).astype(bf16)

    def half_core(j):
        c = cols_of(j)
        s1(j).wait_recv()
        plus(1 - e, away_q, c, r_core[1 - e, away_r, c])
        h1(j).start()
        plus(e, away_q, c, r_core[e, away_r, c])
        plus(1 - e, own_q, c, r_core[1 - e, own_r, c])

    def half_mid(j):
        c = cols_of(j)
        h1(j).wait_recv()
        plus(1 - e, own_q, c, r_half[:, c])
        h3(j).start()
        h2(j).start()

    def half_mate(j):
        c = cols_of(j)
        h3(j).wait_recv()
        part2[e, own_q, c] = (
            part2[e, own_q, c].astype(f32)
            + r_core[e, own_r, c].astype(f32)
            + r_mate[own_r, c].astype(f32)
        ).astype(bf16)
        h4(j).start()

    def mate_sum(j):
        if j < n_half:
            half_mate(j)
            return
        c = cols_of(j)
        s2(j).wait_recv()
        part2[e, mine_h, c] = (
            part2[e, mine_h, c].astype(f32)
            + r_core[e, :, c].astype(f32)
            + r_mate[:, c].astype(f32)
        ).astype(bf16)
        s3(j, 1).start()

    def x_sum(j, b):
        c = cols_of(j)
        s3(j, b - 1).wait()
        part2[e, mine_h, c] = (
            part2[e, mine_h, c].astype(f32) + r_x[b - 2, :, c].astype(f32)
        ).astype(bf16)
        s3(j, b).start()

    stages = [core_sum, mate_sum]
    for b in range(2, bits):
        stages.append(functools.partial(x_sum, b=b))
    n_ch = len(chunks)

    def later_sums(j):
        for i, stage in enumerate(stages[1:]):
            if 0 <= j - i < n_ch:
                stage(j - i)

    def chunk(j):
        if j % sub == sub - 1:
            for q in range(n_pc):
                f_wait(DN, 2 * chunks[j][0] + 1 - p, q)
        product(j)
        if j >= 1:
            core_sum(j - 1)
        if j < n_first and 0 <= j - 2 < n_half:
            half_mid(j - 2)

    n_half = 3 if bits == 2 else 0
    summed = {at_inner: 0, at_end: 0}

    def sums(where, n):
        lo = summed[where]
        stop = n_ch + len(stages) - 2
        hi = min(stop, lo + n)
        summed[where] = hi

        @where
        def _():
            for j in range(lo, hi):
                later_sums(j)

    n_first = 3 * sub
    mids = n_pc if nk > 2 else 0

    def ahead(where, q):
        if 0 <= q < mids:
            where(lambda: relay_some(DN, n_pc + q, n_pc + q + 1))

    for j in range(n_first):
        chunk(j)
        ahead(at_inner, j - 0)
        ahead(at_end, j - 3)
        if j >= 3:
            sums(at_end, 1)
    for j in range(max(0, n_first - 2), n_half):
        half_mid(j)
    for m in range(1, n_l // n_pc):
        for q in range(n_pc):
            if m > 1:
                relay_some(DN, m * n_pc + q, m * n_pc + q + 1)
            else:
                ahead(at_inner, n_first + q - 0)
                ahead(at_end, n_first + q - 3)
            if q < 4:
                sums(at_inner, 1)
            if q < 2:
                sums(at_end, 1)
        for j in range((m + 2) * sub, (m + 3) * sub):
            chunk(j)
    core_sum(n_ch - 1)
    sums(at_inner, n_ch)
    sums(at_end, n_ch)

    n_out = o_send.shape[0]
    piece_rows = hs // n_out
    tile_o = min(piece_rows, 64)

    def out_rows(i):
        return pl.ds(pl.multiple_of(core * hs + i * piece_rows, piece_rows), piece_rows)

    def out_remote(i):
        return remote(
            out.at[out_rows(i)],
            out.at[out_rows(i)],
            o_send.at[i],
            o_recv.at[i],
            {"tp": flip(1)},
        )

    for j in range(n_ch):
        if j < n_half:
            h2_wait(j)
            h4_wait(j)
        else:
            s3(j, last).wait_recv()
    for i in range(n_out):

        @pl.loop(0, piece_rows // tile_o)
        def _(ii):
            lo = i * piece_rows + ii * tile_o
            here = pl.ds(pl.multiple_of(lo, tile_o), tile_o)
            at = pl.ds(pl.multiple_of(core * hs + lo, tile_o), tile_o)
            total = part2[e, at].astype(f32) + r_x[last - 1, here].astype(f32)
            out[at] = layer_norm(
                residual_scale * first[e, at].astype(f32) + total, c_gain[...], c_shift[...]
            ).astype(bf16)

        out_remote(i).start()

    for a in range(6):
        f_drain(a)
    for c in [tok_z, sum_z, to_mate] + tok_g + reduces[0] + reduces[1] + own_g + mate_g:
        c.wait_send()
    for j in range(n_ch):
        s1(j).wait_send()
        if j < n_half:
            for c in (h1(j), h2(j), h3(j), h4(j)):
                c.wait_send()
        else:
            s2(j).wait_send()
            s3(j, last).wait_send()
    for i in range(n_out):
        out_remote(i).wait()


def local(
    tokens,
    gate_outer,
    gate_inner,
    conv_input,
    mixer_output,
    conv_taps,
    mixer_gain,
    mixer_shift,
    up_weight,
    down_weight,
    channel_gain,
    channel_shift,
):
    seq, width = tokens.shape
    rows, units = up_weight.shape
    chans = gate_outer.shape[1]
    half = units // 2
    n_fs = lax.axis_size("fs")
    n_tp = lax.axis_size("tp")
    bits = n_tp.bit_length() - 1
    nk = n_fs // 2
    hc = chans // 2
    sub = 2 if rows % 128 == 0 else 1
    n_ch = nk * sub
    hs = seq // 2
    n_out = 4
    n_pc = min(4, rows // 16)
    hops = 2
    vmem_bytes = 67043328 - 65536
    n_t = bits + 1 + hops * (4 * bits + 2)
    mix = (gate_outer, gate_inner, conv_input, mixer_output)
    if hc % 128:
        mix = tuple(w.reshape(rows, 2, hc).swapaxes(0, 1) for w in mix)
        conv_taps = conv_taps.reshape(-1, 2, hc)
    dma = pltpu.SemaphoreType.DMA
    return pl.pallas_call(
        functools.partial(kernel, n_fs, n_tp, sub, n_pc, hops),
        out_shape=pltpu.VMEM((seq, width), bf16),
        in_specs=[pl.BlockSpec(memory_space=pl.ANY)] * 12,
        out_specs=pl.BlockSpec(memory_space=pltpu.VMEM),
        scratch_shapes=[
            pltpu.VMEM((seq, width), bf16),
            pltpu.VMEM(conv_taps.shape, f32),
            pltpu.VMEM((1, width), f32),
            pltpu.VMEM((1, width), f32),
            pltpu.VMEM((1, width), f32),
            pltpu.VMEM((1, width), f32),
            pltpu.VMEM((4, width, hc), bf16),
            pltpu.VMEM((width, half), bf16),
            pltpu.VMEM((width, half), bf16),
            pltpu.VMEM((seq, width), bf16),
            pltpu.VMEM((2, seq, hc), f32),
            pltpu.VMEM((2, seq + 8, hc), f32),
            pltpu.VMEM((2, seq, hc), bf16),
            pltpu.VMEM((2, seq, width), bf16),
            pltpu.VMEM((2, seq, width), bf16),
            pltpu.VMEM((seq // n_tp, width), bf16),
            pltpu.VMEM((2, seq, width), bf16),
            pltpu.VMEM((2, seq, half), bf16),
            pltpu.VMEM((2, seq, width), bf16),
            pltpu.VMEM((2, hs, width), bf16),
            pltpu.VMEM((hs, width), bf16),
            pltpu.VMEM((bits - 1, hs, width), bf16),
            pltpu.VMEM((hs // 2, width), bf16),
            dma((6, n_pc)),
            dma((6,)),
            dma((6, nk, n_pc)),
            dma((6, nk, n_pc)),
            dma((6, n_fs, n_pc)),
            dma((n_t,)),
            dma((n_t,)),
            dma((n_ch,)),
            dma((n_ch,)),
            dma((n_ch,)),
            dma((n_ch,)),
            dma((bits - 1, n_ch)),
            dma((bits - 1, n_ch)),
            dma((2, n_ch)),
            dma((2, n_ch)),
            dma((n_out,)),
            dma((n_out,)),
        ],
        compiler_params=pltpu.CompilerParams(
            collective_id=0, has_side_effects=True, vmem_limit_bytes=vmem_bytes - 2 * seq * width
        ),
    )(
        tokens,
        *mix,
        conv_taps,
        mixer_gain.reshape(1, width),
        mixer_shift.reshape(1, width),
        up_weight,
        down_weight,
        channel_gain.reshape(1, width),
        channel_shift.reshape(1, width),
    )


def solution(mesh):
    in_specs = (
        P(("rep", "fs"), None),
        P("fs", "tp"),
        P("fs", "tp"),
        P("fs", "tp"),
        P("fs", "tp"),
        P(None, "tp"),
        P(),
        P(),
        P("fs", "tp"),
        P("fs", "tp"),
        P(),
        P(),
    )
    out_specs = P(("rep", "fs"), None)
    return jax.shard_map(local, mesh=mesh, in_specs=in_specs, out_specs=out_specs, check_vma=False)
```

```python
import functools

import jax
import jax.numpy as jnp
from jax import lax
from jax.experimental import pallas as pl
from jax.experimental.pallas import tpu as pltpu
from jax.sharding import PartitionSpec as P

residual_scale = 8.0**0.25
norm_epsilon = 1e-05
MESH = pl.DeviceIdType.MESH
f32 = jnp.float32
bf16 = jnp.bfloat16
NT = (((1,), (1,)), ((), ()))


def layer_norm(values, gain, shift):
    row_mean = jnp.mean(values, -1, keepdims=True)
    centered = values - row_mean
    variance = jnp.mean(centered * centered, -1, keepdims=True)
    return centered * lax.rsqrt(variance + norm_epsilon) * gain + shift


def xor(value, mask):
    bit = 1
    while bit <= mask:
        if mask & bit:
            value = value + bit - 2 * bit * ((value // bit) % 2)
        bit *= 2
    return value


def kernel(
    n_fs,
    n_tp,
    sub,
    n_pc,
    hops,
    tokens_in,
    w_go,
    w_gi,
    w_ci,
    w_mo,
    taps_in,
    m_gain_in,
    m_shift_in,
    w_up,
    w_dn,
    c_gain_in,
    c_shift_in,
    out,
    tokens,
    taps,
    m_gain,
    m_shift,
    c_gain,
    c_shift,
    mix_g,
    up_g,
    dn_g,
    tok_m,
    outer,
    zpad,
    conv,
    part,
    recv,
    r_sum,
    first,
    hidden,
    part2,
    r_core,
    r_mate,
    r_x,
    r_half,
    local_sem,
    in_sem,
    z_sends,
    y_sends,
    f_recv,
    t_send,
    t_recv,
    s1_send,
    s1_recv,
    s2_send,
    s2_recv,
    s3_send,
    s3_recv,
    h_send,
    h_recv,
    o_send,
    o_recv,
):
    seq, width = tokens.shape
    rows = w_up.shape[0]
    half = w_up.shape[1] // 2
    hc = mix_g.shape[2]
    bits = n_tp.bit_length() - 1
    nk = n_fs // 2
    f = lax.axis_index("fs")
    t = lax.axis_index("tp")
    k = f // 2
    p = f % 2
    partner = f + 1 - 2 * p
    e = k % 2
    mate_k = k + 1 - 2 * e
    mate = 2 * mate_k + p
    core = t % 2
    hs = seq // 2
    inner = jnp.logical_and(k > 0, k < nk - 1)

    def flip(bit):
        return t + bit - 2 * bit * ((t // bit) % 2)

    def span(start, n):
        return pl.ds(pl.multiple_of(start, n), n)

    def remote(src, dst, ssem, rsem, device):
        return pltpu.make_async_remote_copy(
            src_ref=src,
            dst_ref=dst,
            send_sem=ssem,
            recv_sem=rsem,
            device_id=device,
            device_id_type=MESH,
        )

    sources = (w_go, w_gi, w_ci, w_mo, w_up, w_dn)
    UP, DN = 4, 5

    def pieces(a):
        return n_pc if a >= UP else 1

    def source(a, parity, q):
        w = sources[a]
        pn = rows // pieces(a)
        at = pl.ds(q * pn, pn)
        if len(w.shape) == 3:
            return w.at[parity, at]
        n = half if a >= UP else hc
        return w.at[at, span(parity * n, n)]

    def held(a, s, q):
        pn = rows // pieces(a)
        at = span(s * rows + q * pn, pn)
        if a < UP:
            return mix_g.at[a, at]
        return (up_g if a == UP else dn_g).at[at]

    copies = []
    for a in range(6):
        for q in range(pieces(a)):
            copies.append(
                pltpu.make_async_copy(source(a, e, q), held(a, f, q), local_sem.at[a, q])
            )
    small = (
        (tokens_in, tokens),
        (taps_in, taps),
        (m_gain_in, m_gain),
        (m_shift_in, m_shift),
        (c_gain_in, c_gain),
        (c_shift_in, c_shift),
    )
    for i, (here, there) in enumerate(small):
        copies.append(pltpu.make_async_copy(here, there, in_sem.at[i]))
    barrier = pltpu.get_barrier_semaphore()
    pl.semaphore_signal(barrier, inc=1, device_id={"fs": partner}, device_id_type=MESH)
    for i in range(1, nk):
        pl.semaphore_signal(
            barrier, inc=1, device_id={"fs": 2 * xor(k, i) + p}, device_id_type=MESH
        )
    for b in range(bits):
        pl.semaphore_signal(barrier, inc=1, device_id={"tp": flip(1 << b)}, device_id_type=MESH)
    for c in copies:
        c.start()
    pl.semaphore_wait(barrier, nk + bits)

    def z_copy(a, to_k, q):
        return remote(
            source(a, to_k % 2, q),
            held(a, f, q),
            z_sends.at[a, to_k, q],
            f_recv.at[a, f, q],
            {"fs": 2 * to_k + p},
        )

    def y_copy(a, of_k, q):
        ref = held(a, 2 * of_k + p, q)
        return remote(
            ref, ref, y_sends.at[a, of_k, q], f_recv.at[a, 2 * of_k + p, q], {"fs": partner}
        )

    def f_wait(a, s, q):
        ref = held(a, s, q)
        remote(ref, ref, y_sends.at[a, 0, q], f_recv.at[a, s, q], {"fs": partner}).wait_recv()

    def z_send(a, kk):
        for q in range(pieces(a)):
            z_copy(a, kk, q).start()

    def z_right(arrays, d, lo=1, hi=None):
        @pl.when(k == d)
        def _():
            for kk in range(d + lo, nk if hi is None else min(d + hi, nk)):
                for a in arrays:
                    z_send(a, kk)

    def z_left(arrays, d, lo=1, hi=None):
        @pl.when(k == d)
        def _():
            for kk in range(d - lo, -1 if hi is None else max(d - hi, -1), -1):
                for a in arrays:
                    z_send(a, kk)

    def z_all(arrays):
        for d in range(nk):
            z_right(arrays, d)
            z_left(arrays, d)

    def z_ends(arrays, lo, hi=None):
        z_right(arrays, 0, lo, hi)
        z_left(arrays, nk - 1, lo, hi)

    def z_mid(arrays, lo=1, hi=None):
        for d in range(1, nk - 1):
            if d < nk - 2:
                z_right(arrays, d, lo, hi)
            if d > 1:
                z_left(arrays, d, lo, hi)

    def z_outward(arrays):
        z_right(arrays, nk - 2)
        z_left(arrays, 1)

    def y_own(a):
        for q in range(pieces(a)):
            y_copy(a, k, q).start()

    def relay(a, of_k, q):
        f_wait(a, 2 * of_k + p, q)
        y_copy(a, of_k, q).start()

    def relay_all(a, of_k):
        for q in range(pieces(a)):
            relay(a, of_k, q)

    def f_drain(a):
        for kk in range(nk):
            for q in range(pieces(a)):
                y_copy(a, kk, q).wait_send()

            @pl.when(k != kk)
            def _(kk=kk):
                for q in range(pieces(a)):
                    z_copy(a, kk, q).wait_send()

    group = k // 2
    order = [2 * group, 2 * group + 1]
    for m in range(1, nk // 2):
        low = (group // (1 << (m.bit_length() - 1))) % 2
        for j in (0, 1):
            order.append(2 * xor(group, m) + low * (1 - j) + (1 - low) * j)
    later = [(of_k, q) for of_k in order[2:] for q in range(n_pc)]

    def relay_some(a, lo, hi):
        for of_k, q in later[lo:hi]:
            relay(a, of_k, q)

    def partners_wait(a):
        for of_k in order:
            for q in range(pieces(a)):
                f_wait(a, 2 * of_k + 1 - p, q)

    def at_inner(fn):
        pl.when(inner)(fn)

    def at_end(fn):
        pl.when(jnp.logical_not(inner))(fn)

    starts = [0]
    for b in range(bits):
        starts.append(starts[-1] + ((t // (1 << b)) % 2) * (seq >> (b + 1)))

    def aways(b):
        return starts[b] + (1 - (t // (1 << b)) % 2) * (seq >> (b + 1))

    n_t = [0]

    def t_copy(src, dst, device):
        i = n_t[0]
        n_t[0] += 1
        return remote(src, dst, t_send.at[i], t_recv.at[i], device)

    def landing(b):
        return seq - (seq >> b)

    class Split:
        def __init__(self, n, make):
            self.parts = [make(n // hops * h, n // hops) for h in range(hops)]

        def start(self):
            for c in self.parts:
                c.start()

        def wait_recv(self):
            for c in self.parts:
                c.wait_recv()

        def wait_send(self):
            for c in self.parts:
                c.wait_send()

    def shift(start, lo, n):
        return pl.ds(pl.multiple_of(start + lo, n), n)

    def reduce_copy(i, b):
        return Split(
            seq >> (b + 1),
            lambda lo, n: t_copy(
                part.at[i, shift(aways(b), lo, n)],
                recv.at[i, pl.ds(landing(b) + lo, n)],
                {"tp": flip(1 << b)},
            ),
        )

    def add_recv(i, b, start, n, origin=None):
        base = landing(b) - (starts[b + 1] if origin is None else origin)
        tile = min(n, 64)

        @pl.loop(0, n // tile)
        def _(j):
            mine = pl.ds(pl.multiple_of(start + j * tile, tile), tile)
            theirs = pl.ds(pl.multiple_of(base + start + j * tile, tile), tile)
            part[i, mine] = (part[i, mine].astype(f32) + recv[i, theirs].astype(f32)).astype(bf16)

    last = bits - 1
    n_own = seq >> bits
    own_rows = span(starts[bits], n_own)

    tok_z = t_copy(tokens_in.at[own_rows], tok_m.at[own_rows], {"fs": mate})
    tok_g = []
    for b in range(bits):
        ref = tok_m.at[span(starts[b + 1], seq >> (b + 1))]
        tok_g.append(t_copy(ref, ref, {"tp": flip(1 << b)}))
    reduces = [[reduce_copy(i, b) for b in range(bits)] for i in (0, 1)]
    sum_z = Split(
        n_own,
        lambda lo, n: t_copy(
            part.at[1, shift(starts[bits], lo, n)], r_sum.at[pl.ds(lo, n)], {"fs": mate}
        ),
    )

    def mate_piece(lo, n):
        ref = first.at[e, shift(starts[bits], lo, n)]
        return t_copy(ref, ref, {"fs": mate})

    to_mate = Split(n_own, mate_piece)
    gathers = []
    for i in (e, 1 - e):
        gathers.append([])
        for b in range(bits):


            def gather_piece(lo, n):
                ref = first.at[i, shift(starts[b + 1], lo, n)]
                return t_copy(ref, ref, {"tp": flip(1 << b)})

            gathers[-1].append(Split(seq >> (b + 1), gather_piece))
    own_g, mate_g = gathers

    ins = (0, 1, 2)
    tok_z.start()
    z_all(ins)
    z_all((3,))
    z_all((UP,))
    for c in copies:
        c.wait()
    for a in range(UP + 1):
        y_own(a)
    tok_z.wait_recv()
    tok_g[last].start()
    for of_k in [mate_k] + order[2:3]:
        for a in ins:
            relay(a, of_k, 0)
    for b in range(last, 0, -1):
        tok_g[b].wait_recv()
        tok_g[b - 1].start()
    for of_k in order[3:]:
        for a in ins:
            relay(a, of_k, 0)
    for of_k in [mate_k] + order[2:]:
        relay(3, of_k, 0)
    tok_g[0].wait_recv()
    for a in ins:
        partners_wait(a)

    at_end(lambda: y_own(DN))

    pad = zpad.shape[1] - seq
    n_taps = taps.shape[0]
    tile = min(256, seq)

    def project(i, x_ref):
        zpad[i, 0:pad] = jnp.zeros((pad, hc), f32)

        @pl.loop(0, seq // tile)
        def _(j):
            at = pl.ds(pl.multiple_of(j * tile, tile), tile)
            x = x_ref[at]
            if hc % 128 == 0:
                w = jnp.concatenate([mix_g[a] for a in ins], axis=1)
                y = jnp.dot(x, w, preferred_element_type=f32)
                ys = [y[:, a * hc : (a + 1) * hc] for a in ins]
            else:
                ys = [jnp.dot(x, mix_g[a], preferred_element_type=f32) for a in ins]
            outer[i, at] = ys[0]
            zpad[i, pl.ds(pl.multiple_of(j * tile + pad, 8), tile)] = ys[1] * ys[2]

        acc = jnp.zeros((seq, hc), f32)
        for j in range(n_taps):
            lo = pad - (n_taps - 1) + j
            acc = acc + tap_rows[j : j + 1] * zpad[i, lo : lo + seq]
        conv[i] = (outer[i] * acc).astype(bf16)

    if len(taps.shape) == 3:
        tap_rows = taps[:, e, :]
    else:
        tap_rows = taps[:, span(e * hc, hc)]
    wide = min(256, width)

    def mix_out(i, start):
        at_rows = span(start, hs)
        lhs = conv[i, at_rows]

        @pl.loop(0, width // wide)
        def _(j):
            at = pl.ds(pl.multiple_of(j * wide, wide), wide)
            part[i, at_rows, at] = lax.dot_general(
                lhs, mix_g[3, at], NT, preferred_element_type=f32
            ).astype(bf16)

    def stage_up(i, b):
        n = seq >> (b + 1)
        reduces[i][b - 1].wait_recv()
        add_recv(i, b - 1, aways(b), n)
        reduces[i][b].start()
        add_recv(i, b - 1, starts[b + 1], n)

    for i, x_ref in ((1, tok_m), (0, tokens)):
        project(i, x_ref)
        if i:
            partners_wait(3)
        mix_out(i, aways(0))
        reduces[i][0].start()
        mix_out(i, starts[1])
        stage_up(i, 1)
    for b in range(2, bits):
        for i in (1, 0):
            stage_up(i, b)

    n_l = len(later)
    early = n_pc // 2

    @at_end
    def _():
        relay_all(UP, mate_k)

    @at_inner
    def _():
        for q in range(0, n_pc):
            relay(UP, mate_k, q)

    at_inner(lambda: relay_some(UP, 0, n_pc))
    for h in range(hops):
        n_h = n_own // hops
        reduces[1][last].parts[h].wait_recv()
        add_recv(1, last, starts[bits] + h * n_h, n_h, starts[bits])
        sum_z.parts[h].start()
    z_mid((DN,), 1, 2)
    at_end(lambda: relay_some(UP, 0, n_pc))
    relay_some(UP, n_pc, n_l)
    at_inner(lambda: y_own(DN))
    reduces[0][last].wait_recv()
    sum_z.wait_recv()
    tile_n = min(n_own, 64)

    @pl.loop(0, n_own // tile_n)
    def _(i):
        at = pl.ds(pl.multiple_of(starts[bits] + i * tile_n, tile_n), tile_n)
        here = pl.ds(pl.multiple_of(i * tile_n, tile_n), tile_n)
        theirs = pl.ds(pl.multiple_of(landing(last) + i * tile_n, tile_n), tile_n)
        total = part[0, at].astype(f32) + recv[0, theirs].astype(f32) + r_sum[here].astype(f32)
        first[e, at] = layer_norm(
            residual_scale * tokens[at].astype(f32) + total, m_gain[...], m_shift[...]
        ).astype(bf16)

    to_mate.start()
    own_g[last].start()
    z_ends((DN,), 1)
    z_mid((DN,), 2)
    for b in range(last, 0, -1):
        own_g[b].wait_recv()
        own_g[b - 1].start()
    z_outward((DN,))
    wide_u = min(256, half)

    def up(q):
        @pl.loop(0, half // wide_u)
        def _(i):
            at = pl.ds(pl.multiple_of(i * wide_u, wide_u), wide_u)
            u = jnp.maximum(jnp.dot(first[q], up_g[:, at], preferred_element_type=f32), 0.0)
            hidden[q, :, at] = (u * u).astype(bf16)

    @at_inner
    def _():
        for h in range(hops):
            to_mate.parts[h].wait_recv()
            mate_g[last].parts[h].start()

    at_inner(lambda: relay_some(DN, 0, n_pc))
    own_g[0].wait_recv()
    partners_wait(UP)
    up(e)

    @at_end
    def _():
        for h in range(hops):
            to_mate.parts[h].wait_recv()
            mate_g[last].parts[h].start()

    at_end(lambda: relay_some(DN, 0, n_pc))
    for q in range(early):
        relay(DN, mate_k, q)
    for b in range(last, 0, -1):
        mate_g[b].wait_recv()
        mate_g[b - 1].start()
    for q in range(early, n_pc):
        relay(DN, mate_k, q)
    mate_g[0].wait_recv()
    up(1 - e)

    cw = 2 * rows // sub
    mine_h = pl.ds(pl.multiple_of(core * hs, hs), hs)
    away_h = pl.ds(pl.multiple_of((1 - core) * hs, hs), hs)
    chunks = []
    for of_k in order[2:3] + order[:2] + order[3:]:
        for i in range(sub):
            side = (p, 1 - p)[i] if sub == 2 else 0
            chunks.append((of_k, (2 * of_k + side) * rows, i))

    def cols_of(j):
        return pl.ds(pl.multiple_of(chunks[j][1], cw), cw)

    def s1(j):
        c = cols_of(j)
        return remote(
            part2.at[:, away_h, c],
            r_core.at[:, :, c],
            s1_send.at[j],
            s1_recv.at[j],
            {"tp": flip(1)},
        )

    def s2(j):
        c = cols_of(j)
        return remote(
            part2.at[1 - e, mine_h, c],
            r_mate.at[:, c],
            s2_send.at[j],
            s2_recv.at[j],
            {"fs": mate},
        )

    def s3(j, b):
        c = cols_of(j)
        return remote(
            part2.at[e, mine_h, c],
            r_x.at[b - 1, :, c],
            s3_send.at[b - 1, j],
            s3_recv.at[b - 1, j],
            {"tp": flip(1 << b)},
        )

    def product(j):
        c = cols_of(j)
        w = dn_g[c]

        @pl.loop(0, 2)
        def _(q):
            part2[q, :, c] = lax.dot_general(
                hidden[q], w, NT, preferred_element_type=f32
            ).astype(bf16)

        s1(j).start()

    def core_sum(j):
        if j < n_half:
            half_core(j)
            return
        c = cols_of(j)
        s1(j).wait_recv()
        part2[1 - e, mine_h, c] = (
            part2[1 - e, mine_h, c].astype(f32) + r_core[1 - e, :, c].astype(f32)
        ).astype(bf16)
        s2(j).start()

    quarter = hs // 2
    bit = (t // 2) % 2
    own_q = shift(core * hs + bit * quarter, 0, quarter)
    away_q = shift(core * hs + (1 - bit) * quarter, 0, quarter)
    own_r = shift(bit * quarter, 0, quarter)
    away_r = shift((1 - bit) * quarter, 0, quarter)

    def h1(j):
        c = cols_of(j)
        return remote(
            part2.at[1 - e, away_q, c],
            r_half.at[:, c],
            h_send.at[0, j],
            h_recv.at[0, j],
            {"tp": flip(2)},
        )

    def h2(j):
        c = cols_of(j)
        return remote(
            part2.at[e, away_q, c],
            r_x.at[0, away_r, c],
            h_send.at[1, j],
            h_recv.at[1, j],
            {"tp": flip(2)},
        )

    def h2_wait(j):
        c = cols_of(j)
        remote(
            part2.at[e, own_q, c],
            r_x.at[0, own_r, c],
            h_send.at[1, j],
            h_recv.at[1, j],
            {"tp": flip(2)},
        ).wait_recv()

    def h3(j):
        c = cols_of(j)
        return remote(
            part2.at[1 - e, own_q, c],
            r_mate.at[own_r, c],
            s2_send.at[j],
            s2_recv.at[j],
            {"fs": mate},
        )

    def h4(j):
        c = cols_of(j)
        return remote(
            part2.at[e, own_q, c],
            r_x.at[0, own_r, c],
            s3_send.at[0, j],
            s3_recv.at[0, j],
            {"tp": flip(2)},
        )

    def h4_wait(j):
        c = cols_of(j)
        remote(
            part2.at[e, away_q, c],
            r_x.at[0, away_r, c],
            s3_send.at[0, j],
            s3_recv.at[0, j],
            {"tp": flip(2)},
        ).wait_recv()

    def plus(i, at, c, other):
        part2[i, at, c] = (part2[i, at, c].astype(f32) + other.astype(f32)).astype(bf16)

    def half_core(j):
        c = cols_of(j)
        s1(j).wait_recv()
        plus(1 - e, away_q, c, r_core[1 - e, away_r, c])
        h1(j).start()
        plus(e, away_q, c, r_core[e, away_r, c])
        plus(1 - e, own_q, c, r_core[1 - e, own_r, c])

    def half_mid(j):
        c = cols_of(j)
        h1(j).wait_recv()
        plus(1 - e, own_q, c, r_half[:, c])
        h3(j).start()
        h2(j).start()

    def half_mate(j):
        c = cols_of(j)
        h3(j).wait_recv()
        part2[e, own_q, c] = (
            part2[e, own_q, c].astype(f32)
            + r_core[e, own_r, c].astype(f32)
            + r_mate[own_r, c].astype(f32)
        ).astype(bf16)
        h4(j).start()

    def mate_sum(j):
        if j < n_half:
            half_mate(j)
            return
        c = cols_of(j)
        s2(j).wait_recv()
        part2[e, mine_h, c] = (
            part2[e, mine_h, c].astype(f32)
            + r_core[e, :, c].astype(f32)
            + r_mate[:, c].astype(f32)
        ).astype(bf16)
        s3(j, 1).start()

    def x_sum(j, b):
        c = cols_of(j)
        s3(j, b - 1).wait()
        part2[e, mine_h, c] = (
            part2[e, mine_h, c].astype(f32) + r_x[b - 2, :, c].astype(f32)
        ).astype(bf16)
        s3(j, b).start()

    stages = [core_sum, mate_sum]
    for b in range(2, bits):
        stages.append(functools.partial(x_sum, b=b))
    n_ch = len(chunks)

    def later_sums(j):
        for i, stage in enumerate(stages[1:]):
            if 0 <= j - i < n_ch:
                stage(j - i)

    def chunk(j):
        if j % sub == sub - 1:
            for q in range(n_pc):
                f_wait(DN, 2 * chunks[j][0] + 1 - p, q)
        product(j)
        if j >= 1:
            core_sum(j - 1)
        if j < n_first and 0 <= j - 2 < n_half:
            half_mid(j - 2)

    n_half = 3 if bits == 2 else 0
    summed = {at_inner: 0, at_end: 0}

    def sums(where, n):
        lo = summed[where]
        stop = n_ch + len(stages) - 2
        hi = min(stop, lo + n)
        summed[where] = hi

        @where
        def _():
            for j in range(lo, hi):
                later_sums(j)

    n_first = 3 * sub
    mids = n_pc if nk > 2 else 0

    def ahead(where, q):
        if 0 <= q < mids:
            where(lambda: relay_some(DN, n_pc + q, n_pc + q + 1))

    for j in range(n_first):
        chunk(j)
        ahead(at_inner, j - 0)
        ahead(at_end, j - 2)
        if j >= 3:
            sums(at_end, 1)
    for j in range(max(0, n_first - 2), n_half):
        half_mid(j)
    for m in range(1, n_l // n_pc):
        for q in range(n_pc):
            if m > 1:
                relay_some(DN, m * n_pc + q, m * n_pc + q + 1)
            else:
                ahead(at_inner, n_first + q - 0)
                ahead(at_end, n_first + q - 2)
            if q < 4:
                sums(at_inner, 1)
            if q < 2:
                sums(at_end, 1)
        for j in range((m + 2) * sub, (m + 3) * sub):
            chunk(j)
    core_sum(n_ch - 1)
    sums(at_inner, n_ch)
    sums(at_end, n_ch)

    n_out = o_send.shape[0]
    piece_rows = hs // n_out
    tile_o = min(piece_rows, 64)

    def out_rows(i):
        return pl.ds(pl.multiple_of(core * hs + i * piece_rows, piece_rows), piece_rows)

    def out_remote(i):
        return remote(
            out.at[out_rows(i)],
            out.at[out_rows(i)],
            o_send.at[i],
            o_recv.at[i],
            {"tp": flip(1)},
        )

    for j in range(n_ch):
        if j < n_half:
            h2_wait(j)
            h4_wait(j)
        else:
            s3(j, last).wait_recv()
    for i in range(n_out):

        @pl.loop(0, piece_rows // tile_o)
        def _(ii):
            lo = i * piece_rows + ii * tile_o
            here = pl.ds(pl.multiple_of(lo, tile_o), tile_o)
            at = pl.ds(pl.multiple_of(core * hs + lo, tile_o), tile_o)
            total = part2[e, at].astype(f32) + r_x[last - 1, here].astype(f32)
            out[at] = layer_norm(
                residual_scale * first[e, at].astype(f32) + total, c_gain[...], c_shift[...]
            ).astype(bf16)

        out_remote(i).start()

    for a in range(6):
        f_drain(a)
    for c in [tok_z, sum_z, to_mate] + tok_g + reduces[0] + reduces[1] + own_g + mate_g:
        c.wait_send()
    for j in range(n_ch):
        s1(j).wait_send()
        if j < n_half:
            for c in (h1(j), h2(j), h3(j), h4(j)):
                c.wait_send()
        else:
            s2(j).wait_send()
            s3(j, last).wait_send()
    for i in range(n_out):
        out_remote(i).wait()


def local(
    tokens,
    gate_outer,
    gate_inner,
    conv_input,
    mixer_output,
    conv_taps,
    mixer_gain,
    mixer_shift,
    up_weight,
    down_weight,
    channel_gain,
    channel_shift,
):
    seq, width = tokens.shape
    rows, units = up_weight.shape
    chans = gate_outer.shape[1]
    half = units // 2
    n_fs = lax.axis_size("fs")
    n_tp = lax.axis_size("tp")
    bits = n_tp.bit_length() - 1
    nk = n_fs // 2
    hc = chans // 2
    sub = 2 if rows % 128 == 0 else 1
    n_ch = nk * sub
    hs = seq // 2
    n_out = 4
    n_pc = min(4, rows // 16)
    hops = 2
    vmem_bytes = 67043328 - 65536
    n_t = bits + 1 + hops * (4 * bits + 2)
    mix = (gate_outer, gate_inner, conv_input, mixer_output)
    if hc % 128:
        mix = tuple(w.reshape(rows, 2, hc).swapaxes(0, 1) for w in mix)
        conv_taps = conv_taps.reshape(-1, 2, hc)
    dma = pltpu.SemaphoreType.DMA
    return pl.pallas_call(
        functools.partial(kernel, n_fs, n_tp, sub, n_pc, hops),
        out_shape=pltpu.VMEM((seq, width), bf16),
        in_specs=[pl.BlockSpec(memory_space=pl.ANY)] * 12,
        out_specs=pl.BlockSpec(memory_space=pltpu.VMEM),
        scratch_shapes=[
            pltpu.VMEM((seq, width), bf16),
            pltpu.VMEM(conv_taps.shape, f32),
            pltpu.VMEM((1, width), f32),
            pltpu.VMEM((1, width), f32),
            pltpu.VMEM((1, width), f32),
            pltpu.VMEM((1, width), f32),
            pltpu.VMEM((4, width, hc), bf16),
            pltpu.VMEM((width, half), bf16),
            pltpu.VMEM((width, half), bf16),
            pltpu.VMEM((seq, width), bf16),
            pltpu.VMEM((2, seq, hc), f32),
            pltpu.VMEM((2, seq + 8, hc), f32),
            pltpu.VMEM((2, seq, hc), bf16),
            pltpu.VMEM((2, seq, width), bf16),
            pltpu.VMEM((2, seq, width), bf16),
            pltpu.VMEM((seq // n_tp, width), bf16),
            pltpu.VMEM((2, seq, width), bf16),
            pltpu.VMEM((2, seq, half), bf16),
            pltpu.VMEM((2, seq, width), bf16),
            pltpu.VMEM((2, hs, width), bf16),
            pltpu.VMEM((hs, width), bf16),
            pltpu.VMEM((bits - 1, hs, width), bf16),
            pltpu.VMEM((hs // 2, width), bf16),
            dma((6, n_pc)),
            dma((6,)),
            dma((6, nk, n_pc)),
            dma((6, nk, n_pc)),
            dma((6, n_fs, n_pc)),
            dma((n_t,)),
            dma((n_t,)),
            dma((n_ch,)),
            dma((n_ch,)),
            dma((n_ch,)),
            dma((n_ch,)),
            dma((bits - 1, n_ch)),
            dma((bits - 1, n_ch)),
            dma((2, n_ch)),
            dma((2, n_ch)),
            dma((n_out,)),
            dma((n_out,)),
        ],
        compiler_params=pltpu.CompilerParams(
            collective_id=0, has_side_effects=True, vmem_limit_bytes=vmem_bytes - 2 * seq * width
        ),
    )(
        tokens,
        *mix,
        conv_taps,
        mixer_gain.reshape(1, width),
        mixer_shift.reshape(1, width),
        up_weight,
        down_weight,
        channel_gain.reshape(1, width),
        channel_shift.reshape(1, width),
    )


def solution(mesh):
    in_specs = (
        P(("rep", "fs"), None),
        P("fs", "tp"),
        P("fs", "tp"),
        P("fs", "tp"),
        P("fs", "tp"),
        P(None, "tp"),
        P(),
        P(),
        P("fs", "tp"),
        P("fs", "tp"),
        P(),
        P(),
    )
    out_specs = P(("rep", "fs"), None)
    return jax.shard_map(local, mesh=mesh, in_specs=in_specs, out_specs=out_specs, check_vma=False)
```

```python
import functools

import jax
import jax.numpy as jnp
from jax import lax
from jax.experimental import pallas as pl
from jax.experimental.pallas import tpu as pltpu
from jax.sharding import PartitionSpec as P

residual_scale = 8.0**0.25
norm_epsilon = 1e-05
MESH = pl.DeviceIdType.MESH
f32 = jnp.float32
bf16 = jnp.bfloat16
NT = (((1,), (1,)), ((), ()))


def layer_norm(values, gain, shift):
    row_mean = jnp.mean(values, -1, keepdims=True)
    centered = values - row_mean
    variance = jnp.mean(centered * centered, -1, keepdims=True)
    return centered * lax.rsqrt(variance + norm_epsilon) * gain + shift


def xor(value, mask):
    bit = 1
    while bit <= mask:
        if mask & bit:
            value = value + bit - 2 * bit * ((value // bit) % 2)
        bit *= 2
    return value


def kernel(
    n_fs,
    n_tp,
    sub,
    n_pc,
    hops,
    tokens_in,
    w_go,
    w_gi,
    w_ci,
    w_mo,
    taps_in,
    m_gain_in,
    m_shift_in,
    w_up,
    w_dn,
    c_gain_in,
    c_shift_in,
    out,
    tokens,
    taps,
    m_gain,
    m_shift,
    c_gain,
    c_shift,
    mix_g,
    up_g,
    dn_g,
    tok_m,
    outer,
    zpad,
    conv,
    part,
    recv,
    r_sum,
    first,
    hidden,
    part2,
    r_core,
    r_mate,
    r_x,
    r_half,
    local_sem,
    in_sem,
    z_sends,
    y_sends,
    f_recv,
    t_send,
    t_recv,
    s1_send,
    s1_recv,
    s2_send,
    s2_recv,
    s3_send,
    s3_recv,
    h_send,
    h_recv,
    o_send,
    o_recv,
):
    seq, width = tokens.shape
    rows = w_up.shape[0]
    half = w_up.shape[1] // 2
    hc = mix_g.shape[2]
    bits = n_tp.bit_length() - 1
    nk = n_fs // 2
    f = lax.axis_index("fs")
    t = lax.axis_index("tp")
    k = f // 2
    p = f % 2
    partner = f + 1 - 2 * p
    e = k % 2
    mate_k = k + 1 - 2 * e
    mate = 2 * mate_k + p
    core = t % 2
    hs = seq // 2
    inner = jnp.logical_and(k > 0, k < nk - 1)

    def flip(bit):
        return t + bit - 2 * bit * ((t // bit) % 2)

    def span(start, n):
        return pl.ds(pl.multiple_of(start, n), n)

    def remote(src, dst, ssem, rsem, device):
        return pltpu.make_async_remote_copy(
            src_ref=src,
            dst_ref=dst,
            send_sem=ssem,
            recv_sem=rsem,
            device_id=device,
            device_id_type=MESH,
        )

    sources = (w_go, w_gi, w_ci, w_mo, w_up, w_dn)
    UP, DN = 4, 5

    def pieces(a):
        return n_pc if a >= UP else 1

    def source(a, parity, q):
        w = sources[a]
        pn = rows // pieces(a)
        at = pl.ds(q * pn, pn)
        if len(w.shape) == 3:
            return w.at[parity, at]
        n = half if a >= UP else hc
        return w.at[at, span(parity * n, n)]

    def held(a, s, q):
        pn = rows // pieces(a)
        at = span(s * rows + q * pn, pn)
        if a < UP:
            return mix_g.at[a, at]
        return (up_g if a == UP else dn_g).at[at]

    copies = []
    for a in range(6):
        for q in range(pieces(a)):
            copies.append(
                pltpu.make_async_copy(source(a, e, q), held(a, f, q), local_sem.at[a, q])
            )
    small = (
        (tokens_in, tokens),
        (taps_in, taps),
        (m_gain_in, m_gain),
        (m_shift_in, m_shift),
        (c_gain_in, c_gain),
        (c_shift_in, c_shift),
    )
    for i, (here, there) in enumerate(small):
        copies.append(pltpu.make_async_copy(here, there, in_sem.at[i]))
    barrier = pltpu.get_barrier_semaphore()
    pl.semaphore_signal(barrier, inc=1, device_id={"fs": partner}, device_id_type=MESH)
    for i in range(1, nk):
        pl.semaphore_signal(
            barrier, inc=1, device_id={"fs": 2 * xor(k, i) + p}, device_id_type=MESH
        )
    for b in range(bits):
        pl.semaphore_signal(barrier, inc=1, device_id={"tp": flip(1 << b)}, device_id_type=MESH)
    for c in copies:
        c.start()
    pl.semaphore_wait(barrier, nk + bits)

    def z_copy(a, to_k, q):
        return remote(
            source(a, to_k % 2, q),
            held(a, f, q),
            z_sends.at[a, to_k, q],
            f_recv.at[a, f, q],
            {"fs": 2 * to_k + p},
        )

    def y_copy(a, of_k, q):
        ref = held(a, 2 * of_k + p, q)
        return remote(
            ref, ref, y_sends.at[a, of_k, q], f_recv.at[a, 2 * of_k + p, q], {"fs": partner}
        )

    def f_wait(a, s, q):
        ref = held(a, s, q)
        remote(ref, ref, y_sends.at[a, 0, q], f_recv.at[a, s, q], {"fs": partner}).wait_recv()

    def z_send(a, kk):
        for q in range(pieces(a)):
            z_copy(a, kk, q).start()

    def z_right(arrays, d, lo=1, hi=None):
        @pl.when(k == d)
        def _():
            for kk in range(d + lo, nk if hi is None else min(d + hi, nk)):
                for a in arrays:
                    z_send(a, kk)

    def z_left(arrays, d, lo=1, hi=None):
        @pl.when(k == d)
        def _():
            for kk in range(d - lo, -1 if hi is None else max(d - hi, -1), -1):
                for a in arrays:
                    z_send(a, kk)

    def z_all(arrays):
        for d in range(nk):
            z_right(arrays, d)
            z_left(arrays, d)

    def z_ends(arrays, lo, hi=None):
        z_right(arrays, 0, lo, hi)
        z_left(arrays, nk - 1, lo, hi)

    def z_mid(arrays, lo=1, hi=None):
        for d in range(1, nk - 1):
            if d < nk - 2:
                z_right(arrays, d, lo, hi)
            if d > 1:
                z_left(arrays, d, lo, hi)

    def z_outward(arrays):
        z_right(arrays, nk - 2)
        z_left(arrays, 1)

    def y_own(a):
        for q in range(pieces(a)):
            y_copy(a, k, q).start()

    def relay(a, of_k, q):
        f_wait(a, 2 * of_k + p, q)
        y_copy(a, of_k, q).start()

    def relay_all(a, of_k):
        for q in range(pieces(a)):
            relay(a, of_k, q)

    def f_drain(a):
        for kk in range(nk):
            for q in range(pieces(a)):
                y_copy(a, kk, q).wait_send()

            @pl.when(k != kk)
            def _(kk=kk):
                for q in range(pieces(a)):
                    z_copy(a, kk, q).wait_send()

    group = k // 2
    order = [2 * group, 2 * group + 1]
    for m in range(1, nk // 2):
        low = (group // (1 << (m.bit_length() - 1))) % 2
        for j in (0, 1):
            order.append(2 * xor(group, m) + low * (1 - j) + (1 - low) * j)
    later = [(of_k, q) for of_k in order[2:] for q in range(n_pc)]

    def relay_some(a, lo, hi):
        for of_k, q in later[lo:hi]:
            relay(a, of_k, q)

    def partners_wait(a):
        for of_k in order:
            for q in range(pieces(a)):
                f_wait(a, 2 * of_k + 1 - p, q)

    def at_inner(fn):
        pl.when(inner)(fn)

    def at_end(fn):
        pl.when(jnp.logical_not(inner))(fn)

    starts = [0]
    for b in range(bits):
        starts.append(starts[-1] + ((t // (1 << b)) % 2) * (seq >> (b + 1)))

    def aways(b):
        return starts[b] + (1 - (t // (1 << b)) % 2) * (seq >> (b + 1))

    n_t = [0]

    def t_copy(src, dst, device):
        i = n_t[0]
        n_t[0] += 1
        return remote(src, dst, t_send.at[i], t_recv.at[i], device)

    def landing(b):
        return seq - (seq >> b)

    class Split:
        def __init__(self, n, make):
            self.parts = [make(n // hops * h, n // hops) for h in range(hops)]

        def start(self):
            for c in self.parts:
                c.start()

        def wait_recv(self):
            for c in self.parts:
                c.wait_recv()

        def wait_send(self):
            for c in self.parts:
                c.wait_send()

    def shift(start, lo, n):
        return pl.ds(pl.multiple_of(start + lo, n), n)

    def reduce_copy(i, b):
        return Split(
            seq >> (b + 1),
            lambda lo, n: t_copy(
                part.at[i, shift(aways(b), lo, n)],
                recv.at[i, pl.ds(landing(b) + lo, n)],
                {"tp": flip(1 << b)},
            ),
        )

    def add_recv(i, b, start, n, origin=None):
        base = landing(b) - (starts[b + 1] if origin is None else origin)
        tile = min(n, 64)

        @pl.loop(0, n // tile)
        def _(j):
            mine = pl.ds(pl.multiple_of(start + j * tile, tile), tile)
            theirs = pl.ds(pl.multiple_of(base + start + j * tile, tile), tile)
            part[i, mine] = (part[i, mine].astype(f32) + recv[i, theirs].astype(f32)).astype(bf16)

    last = bits - 1
    n_own = seq >> bits
    own_rows = span(starts[bits], n_own)

    tok_z = t_copy(tokens_in.at[own_rows], tok_m.at[own_rows], {"fs": mate})
    tok_g = []
    for b in range(bits):
        ref = tok_m.at[span(starts[b + 1], seq >> (b + 1))]
        tok_g.append(t_copy(ref, ref, {"tp": flip(1 << b)}))
    reduces = [[reduce_copy(i, b) for b in range(bits)] for i in (0, 1)]
    sum_z = Split(
        n_own,
        lambda lo, n: t_copy(
            part.at[1, shift(starts[bits], lo, n)], r_sum.at[pl.ds(lo, n)], {"fs": mate}
        ),
    )

    def mate_piece(lo, n):
        ref = first.at[e, shift(starts[bits], lo, n)]
        return t_copy(ref, ref, {"fs": mate})

    to_mate = Split(n_own, mate_piece)
    gathers = []
    for i in (e, 1 - e):
        gathers.append([])
        for b in range(bits):


            def gather_piece(lo, n):
                ref = first.at[i, shift(starts[b + 1], lo, n)]
                return t_copy(ref, ref, {"tp": flip(1 << b)})

            gathers[-1].append(Split(seq >> (b + 1), gather_piece))
    own_g, mate_g = gathers

    ins = (0, 1, 2)
    tok_z.start()
    z_all(ins)
    z_all((3,))
    z_all((UP,))
    for c in copies:
        c.wait()
    for a in range(UP + 1):
        y_own(a)
    tok_z.wait_recv()
    tok_g[last].start()
    for of_k in [mate_k] + order[2:3]:
        for a in ins:
            relay(a, of_k, 0)
    for b in range(last, 0, -1):
        tok_g[b].wait_recv()
        tok_g[b - 1].start()
    for of_k in order[3:]:
        for a in ins:
            relay(a, of_k, 0)
    for of_k in [mate_k] + order[2:]:
        relay(3, of_k, 0)
    tok_g[0].wait_recv()
    for a in ins:
        partners_wait(a)

    at_end(lambda: y_own(DN))

    pad = zpad.shape[1] - seq
    n_taps = taps.shape[0]
    tile = min(256, seq)

    def project(i, x_ref):
        zpad[i, 0:pad] = jnp.zeros((pad, hc), f32)

        @pl.loop(0, seq // tile)
        def _(j):
            at = pl.ds(pl.multiple_of(j * tile, tile), tile)
            x = x_ref[at]
            if hc % 128 == 0:
                w = jnp.concatenate([mix_g[a] for a in ins], axis=1)
                y = jnp.dot(x, w, preferred_element_type=f32)
                ys = [y[:, a * hc : (a + 1) * hc] for a in ins]
            else:
                ys = [jnp.dot(x, mix_g[a], preferred_element_type=f32) for a in ins]
            outer[i, at] = ys[0]
            zpad[i, pl.ds(pl.multiple_of(j * tile + pad, 8), tile)] = ys[1] * ys[2]

        acc = jnp.zeros((seq, hc), f32)
        for j in range(n_taps):
            lo = pad - (n_taps - 1) + j
            acc = acc + tap_rows[j : j + 1] * zpad[i, lo : lo + seq]
        conv[i] = (outer[i] * acc).astype(bf16)

    if len(taps.shape) == 3:
        tap_rows = taps[:, e, :]
    else:
        tap_rows = taps[:, span(e * hc, hc)]
    wide = min(256, width)

    def mix_out(i, start):
        at_rows = span(start, hs)
        lhs = conv[i, at_rows]

        @pl.loop(0, width // wide)
        def _(j):
            at = pl.ds(pl.multiple_of(j * wide, wide), wide)
            part[i, at_rows, at] = lax.dot_general(
                lhs, mix_g[3, at], NT, preferred_element_type=f32
            ).astype(bf16)

    def stage_up(i, b):
        n = seq >> (b + 1)
        reduces[i][b - 1].wait_recv()
        add_recv(i, b - 1, aways(b), n)
        reduces[i][b].start()
        add_recv(i, b - 1, starts[b + 1], n)

    for i, x_ref in ((1, tok_m), (0, tokens)):
        project(i, x_ref)
        if i:
            partners_wait(3)
        mix_out(i, aways(0))
        reduces[i][0].start()
        mix_out(i, starts[1])
        stage_up(i, 1)
    for b in range(2, bits):
        for i in (1, 0):
            stage_up(i, b)

    n_l = len(later)
    early = n_pc // 2

    @at_end
    def _():
        relay_all(UP, mate_k)

    @at_inner
    def _():
        for q in range(0, n_pc):
            relay(UP, mate_k, q)

    at_inner(lambda: relay_some(UP, 0, n_pc))
    for h in range(hops):
        n_h = n_own // hops
        reduces[1][last].parts[h].wait_recv()
        add_recv(1, last, starts[bits] + h * n_h, n_h, starts[bits])
        sum_z.parts[h].start()
    z_mid((DN,), 1, 2)
    at_end(lambda: relay_some(UP, 0, n_pc))
    relay_some(UP, n_pc, n_l)
    at_inner(lambda: y_own(DN))
    reduces[0][last].wait_recv()
    sum_z.wait_recv()
    tile_n = min(n_own, 64)

    @pl.loop(0, n_own // tile_n)
    def _(i):
        at = pl.ds(pl.multiple_of(starts[bits] + i * tile_n, tile_n), tile_n)
        here = pl.ds(pl.multiple_of(i * tile_n, tile_n), tile_n)
        theirs = pl.ds(pl.multiple_of(landing(last) + i * tile_n, tile_n), tile_n)
        total = part[0, at].astype(f32) + recv[0, theirs].astype(f32) + r_sum[here].astype(f32)
        first[e, at] = layer_norm(
            residual_scale * tokens[at].astype(f32) + total, m_gain[...], m_shift[...]
        ).astype(bf16)

    to_mate.start()
    own_g[last].start()
    z_ends((DN,), 1)
    z_mid((DN,), 2)
    for b in range(last, 0, -1):
        own_g[b].wait_recv()
        own_g[b - 1].start()
    z_outward((DN,))
    wide_u = min(256, half)

    def up(q):
        @pl.loop(0, half // wide_u)
        def _(i):
            at = pl.ds(pl.multiple_of(i * wide_u, wide_u), wide_u)
            u = jnp.maximum(jnp.dot(first[q], up_g[:, at], preferred_element_type=f32), 0.0)
            hidden[q, :, at] = (u * u).astype(bf16)

    @at_inner
    def _():
        for h in range(hops):
            to_mate.parts[h].wait_recv()
            mate_g[last].parts[h].start()

    at_inner(lambda: relay_some(DN, 0, n_pc))
    own_g[0].wait_recv()
    partners_wait(UP)
    up(e)

    @at_end
    def _():
        for h in range(hops):
            to_mate.parts[h].wait_recv()
            mate_g[last].parts[h].start()

    at_end(lambda: relay_some(DN, 0, n_pc))
    for q in range(early):
        relay(DN, mate_k, q)
    for b in range(last, 0, -1):
        mate_g[b].wait_recv()
        mate_g[b - 1].start()
    for q in range(early, n_pc):
        relay(DN, mate_k, q)
    mate_g[0].wait_recv()
    up(1 - e)

    cw = 2 * rows // sub
    mine_h = pl.ds(pl.multiple_of(core * hs, hs), hs)
    away_h = pl.ds(pl.multiple_of((1 - core) * hs, hs), hs)
    chunks = []
    for of_k in order[2:3] + order[:2] + order[3:]:
        for i in range(sub):
            side = (p, 1 - p)[i] if sub == 2 else 0
            chunks.append((of_k, (2 * of_k + side) * rows, i))

    def cols_of(j):
        return pl.ds(pl.multiple_of(chunks[j][1], cw), cw)

    def s1(j):
        c = cols_of(j)
        return remote(
            part2.at[:, away_h, c],
            r_core.at[:, :, c],
            s1_send.at[j],
            s1_recv.at[j],
            {"tp": flip(1)},
        )

    def s2(j):
        c = cols_of(j)
        return remote(
            part2.at[1 - e, mine_h, c],
            r_mate.at[:, c],
            s2_send.at[j],
            s2_recv.at[j],
            {"fs": mate},
        )

    def s3(j, b):
        c = cols_of(j)
        return remote(
            part2.at[e, mine_h, c],
            r_x.at[b - 1, :, c],
            s3_send.at[b - 1, j],
            s3_recv.at[b - 1, j],
            {"tp": flip(1 << b)},
        )

    def product(j):
        c = cols_of(j)
        w = dn_g[c]

        @pl.loop(0, 2)
        def _(q):
            part2[q, :, c] = lax.dot_general(
                hidden[q], w, NT, preferred_element_type=f32
            ).astype(bf16)

        s1(j).start()

    def core_sum(j):
        if j < n_half:
            half_core(j)
            return
        c = cols_of(j)
        s1(j).wait_recv()
        part2[1 - e, mine_h, c] = (
            part2[1 - e, mine_h, c].astype(f32) + r_core[1 - e, :, c].astype(f32)
        ).astype(bf16)
        s2(j).start()

    quarter = hs // 2
    bit = (t // 2) % 2
    own_q = shift(core * hs + bit * quarter, 0, quarter)
    away_q = shift(core * hs + (1 - bit) * quarter, 0, quarter)
    own_r = shift(bit * quarter, 0, quarter)
    away_r = shift((1 - bit) * quarter, 0, quarter)

    def h1(j):
        c = cols_of(j)
        return remote(
            part2.at[1 - e, away_q, c],
            r_half.at[:, c],
            h_send.at[0, j],
            h_recv.at[0, j],
            {"tp": flip(2)},
        )

    def h2(j):
        c = cols_of(j)
        return remote(
            part2.at[e, away_q, c],
            r_x.at[0, away_r, c],
            h_send.at[1, j],
            h_recv.at[1, j],
            {"tp": flip(2)},
        )

    def h2_wait(j):
        c = cols_of(j)
        remote(
            part2.at[e, own_q, c],
            r_x.at[0, own_r, c],
            h_send.at[1, j],
            h_recv.at[1, j],
            {"tp": flip(2)},
        ).wait_recv()

    def h3(j):
        c = cols_of(j)
        return remote(
            part2.at[1 - e, own_q, c],
            r_mate.at[own_r, c],
            s2_send.at[j],
            s2_recv.at[j],
            {"fs": mate},
        )

    def h4(j):
        c = cols_of(j)
        return remote(
            part2.at[e, own_q, c],
            r_x.at[0, own_r, c],
            s3_send.at[0, j],
            s3_recv.at[0, j],
            {"tp": flip(2)},
        )

    def h4_wait(j):
        c = cols_of(j)
        remote(
            part2.at[e, away_q, c],
            r_x.at[0, away_r, c],
            s3_send.at[0, j],
            s3_recv.at[0, j],
            {"tp": flip(2)},
        ).wait_recv()

    def plus(i, at, c, other):
        part2[i, at, c] = (part2[i, at, c].astype(f32) + other.astype(f32)).astype(bf16)

    def half_core(j):
        c = cols_of(j)
        s1(j).wait_recv()
        plus(1 - e, away_q, c, r_core[1 - e, away_r, c])
        h1(j).start()
        plus(e, away_q, c, r_core[e, away_r, c])
        plus(1 - e, own_q, c, r_core[1 - e, own_r, c])

    def half_mid(j):
        c = cols_of(j)
        h1(j).wait_recv()
        plus(1 - e, own_q, c, r_half[:, c])
        h3(j).start()
        h2(j).start()

    def half_mate(j):
        c = cols_of(j)
        h3(j).wait_recv()
        part2[e, own_q, c] = (
            part2[e, own_q, c].astype(f32)
            + r_core[e, own_r, c].astype(f32)
            + r_mate[own_r, c].astype(f32)
        ).astype(bf16)
        h4(j).start()

    def mate_sum(j):
        if j < n_half:
            half_mate(j)
            return
        c = cols_of(j)
        s2(j).wait_recv()
        part2[e, mine_h, c] = (
            part2[e, mine_h, c].astype(f32)
            + r_core[e, :, c].astype(f32)
            + r_mate[:, c].astype(f32)
        ).astype(bf16)
        s3(j, 1).start()

    def x_sum(j, b):
        c = cols_of(j)
        s3(j, b - 1).wait()
        part2[e, mine_h, c] = (
            part2[e, mine_h, c].astype(f32) + r_x[b - 2, :, c].astype(f32)
        ).astype(bf16)
        s3(j, b).start()

    stages = [core_sum, mate_sum]
    for b in range(2, bits):
        stages.append(functools.partial(x_sum, b=b))
    n_ch = len(chunks)

    def later_sums(j):
        for i, stage in enumerate(stages[1:]):
            if 0 <= j - i < n_ch:
                stage(j - i)

    def chunk(j):
        if j % sub == sub - 1:
            for q in range(n_pc):
                f_wait(DN, 2 * chunks[j][0] + 1 - p, q)
        product(j)
        if j >= 1:
            core_sum(j - 1)
        if j < n_first and 0 <= j - 2 < n_half:
            half_mid(j - 2)

    n_half = 3 if bits == 2 else 0
    summed = {at_inner: 0, at_end: 0}

    def sums(where, n):
        lo = summed[where]
        stop = n_ch + len(stages) - 2
        hi = min(stop, lo + n)
        summed[where] = hi

        @where
        def _():
            for j in range(lo, hi):
                later_sums(j)

    n_first = 3 * sub
    mids = n_pc if nk > 2 else 0

    def ahead(where, q):
        if 0 <= q < mids:
            where(lambda: relay_some(DN, n_pc + q, n_pc + q + 1))

    for j in range(n_first):
        chunk(j)
        ahead(at_inner, j - 0)
        ahead(at_end, j - 2)
        if j >= 3:
            sums(at_end, 1)
    for j in range(max(0, n_first - 2), n_half):
        half_mid(j)
    for m in range(1, n_l // n_pc):
        for q in range(n_pc):
            if m > 1:
                relay_some(DN, m * n_pc + q, m * n_pc + q + 1)
            else:
                ahead(at_inner, n_first + q - 0)
                ahead(at_end, n_first + q - 2)
            if q < 4:
                sums(at_inner, 1)
            if q < 2:
                sums(at_end, 1)
        for j in range((m + 2) * sub, (m + 3) * sub):
            chunk(j)
    core_sum(n_ch - 1)
    sums(at_inner, n_ch)
    sums(at_end, n_ch)

    n_out = o_send.shape[0]
    piece_rows = hs // n_out
    tile_o = min(piece_rows, 64)

    def out_rows(i):
        return pl.ds(pl.multiple_of(core * hs + i * piece_rows, piece_rows), piece_rows)

    def out_remote(i):
        return remote(
            out.at[out_rows(i)],
            out.at[out_rows(i)],
            o_send.at[i],
            o_recv.at[i],
            {"tp": flip(1)},
        )

    for j in range(n_ch):
        if j < n_half:
            h2_wait(j)
            h4_wait(j)
        else:
            s3(j, last).wait_recv()
    for i in range(n_out):

        @pl.loop(0, piece_rows // tile_o)
        def _(ii):
            lo = i * piece_rows + ii * tile_o
            here = pl.ds(pl.multiple_of(lo, tile_o), tile_o)
            at = pl.ds(pl.multiple_of(core * hs + lo, tile_o), tile_o)
            total = part2[e, at].astype(f32) + r_x[last - 1, here].astype(f32)
            out[at] = layer_norm(
                residual_scale * first[e, at].astype(f32) + total, c_gain[...], c_shift[...]
            ).astype(bf16)

        out_remote(i).start()

    for a in range(6):
        f_drain(a)
    for c in [tok_z, sum_z, to_mate] + tok_g + reduces[0] + reduces[1] + own_g + mate_g:
        c.wait_send()
    for j in range(n_ch):
        s1(j).wait_send()
        if j < n_half:
            for c in (h1(j), h2(j), h3(j), h4(j)):
                c.wait_send()
        else:
            s2(j).wait_send()
            s3(j, last).wait_send()
    for i in range(n_out):
        out_remote(i).wait()


def local(
    tokens,
    gate_outer,
    gate_inner,
    conv_input,
    mixer_output,
    conv_taps,
    mixer_gain,
    mixer_shift,
    up_weight,
    down_weight,
    channel_gain,
    channel_shift,
):
    seq, width = tokens.shape
    rows, units = up_weight.shape
    chans = gate_outer.shape[1]
    half = units // 2
    n_fs = lax.axis_size("fs")
    n_tp = lax.axis_size("tp")
    bits = n_tp.bit_length() - 1
    nk = n_fs // 2
    hc = chans // 2
    sub = 2 if rows % 128 == 0 else 1
    n_ch = nk * sub
    hs = seq // 2
    n_out = 4
    n_pc = min(2, rows // 16)
    hops = 2
    vmem_bytes = 67043328 - 65536
    n_t = bits + 1 + hops * (4 * bits + 2)
    mix = (gate_outer, gate_inner, conv_input, mixer_output)
    if hc % 128:
        mix = tuple(w.reshape(rows, 2, hc).swapaxes(0, 1) for w in mix)
        conv_taps = conv_taps.reshape(-1, 2, hc)
    dma = pltpu.SemaphoreType.DMA
    return pl.pallas_call(
        functools.partial(kernel, n_fs, n_tp, sub, n_pc, hops),
        out_shape=pltpu.VMEM((seq, width), bf16),
        in_specs=[pl.BlockSpec(memory_space=pl.ANY)] * 12,
        out_specs=pl.BlockSpec(memory_space=pltpu.VMEM),
        scratch_shapes=[
            pltpu.VMEM((seq, width), bf16),
            pltpu.VMEM(conv_taps.shape, f32),
            pltpu.VMEM((1, width), f32),
            pltpu.VMEM((1, width), f32),
            pltpu.VMEM((1, width), f32),
            pltpu.VMEM((1, width), f32),
            pltpu.VMEM((4, width, hc), bf16),
            pltpu.VMEM((width, half), bf16),
            pltpu.VMEM((width, half), bf16),
            pltpu.VMEM((seq, width), bf16),
            pltpu.VMEM((2, seq, hc), f32),
            pltpu.VMEM((2, seq + 8, hc), f32),
            pltpu.VMEM((2, seq, hc), bf16),
            pltpu.VMEM((2, seq, width), bf16),
            pltpu.VMEM((2, seq, width), bf16),
            pltpu.VMEM((seq // n_tp, width), bf16),
            pltpu.VMEM((2, seq, width), bf16),
            pltpu.VMEM((2, seq, half), bf16),
            pltpu.VMEM((2, seq, width), bf16),
            pltpu.VMEM((2, hs, width), bf16),
            pltpu.VMEM((hs, width), bf16),
            pltpu.VMEM((bits - 1, hs, width), bf16),
            pltpu.VMEM((hs // 2, width), bf16),
            dma((6, n_pc)),
            dma((6,)),
            dma((6, nk, n_pc)),
            dma((6, nk, n_pc)),
            dma((6, n_fs, n_pc)),
            dma((n_t,)),
            dma((n_t,)),
            dma((n_ch,)),
            dma((n_ch,)),
            dma((n_ch,)),
            dma((n_ch,)),
            dma((bits - 1, n_ch)),
            dma((bits - 1, n_ch)),
            dma((2, n_ch)),
            dma((2, n_ch)),
            dma((n_out,)),
            dma((n_out,)),
        ],
        compiler_params=pltpu.CompilerParams(
            collective_id=0, has_side_effects=True, vmem_limit_bytes=vmem_bytes - 2 * seq * width
        ),
    )(
        tokens,
        *mix,
        conv_taps,
        mixer_gain.reshape(1, width),
        mixer_shift.reshape(1, width),
        up_weight,
        down_weight,
        channel_gain.reshape(1, width),
        channel_shift.reshape(1, width),
    )


def solution(mesh):
    in_specs = (
        P(("rep", "fs"), None),
        P("fs", "tp"),
        P("fs", "tp"),
        P("fs", "tp"),
        P("fs", "tp"),
        P(None, "tp"),
        P(),
        P(),
        P("fs", "tp"),
        P("fs", "tp"),
        P(),
        P(),
    )
    out_specs = P(("rep", "fs"), None)
    return jax.shard_map(local, mesh=mesh, in_specs=in_specs, out_specs=out_specs, check_vma=False)
```
